32 devices in a mesh: sp: 8 (over z, x), tp: 4 (over y, core).
Axes of the slice: x: 2, y: 2, z: 4, core: 2. Of those that a mesh axis runs over, the one named last changes fastest.
Arguments:
- stream: bfloat16 [1024, 2048], P('sp', 'tp')
- norm_gain: float32 [2048], P('tp'), may hold values from 0.1 to 1.9
- w_value: bfloat16 [2048, 512], P(None, 'tp'), may hold values from -0.125 to 0.125
- w_mix: bfloat16 [2048, 512], P(None, 'tp'), may hold values from -0.125 to 0.125
- w_gate: bfloat16 [2048, 512], P(None, 'tp'), may hold values from -0.125 to 0.125
- w_state: bfloat16 [2048, 512], P(None, 'tp'), may hold values from -0.125 to 0.125
- conv_taps: float32 [3, 512], P(None, 'tp'), may hold values from -3 to 3
- skip_gain: float32 [512], P('tp'), may hold values from -3 to 3
- decay_rate: float32 [2, 32, 64], P(None, 'tp'), as said below
- turn_rate: float32 [2, 32, 64], P(None, 'tp'), may hold values from 0.25 to 1.5
- input_real: float32 [2, 32, 64, 16], P(None, 'tp')
- input_imag: float32 [2, 32, 64, 16], P(None, 'tp')
- read_real: float32 [2, 32, 16, 64], P(None, 'tp'), may hold values from -0.75 to 0.75
- read_imag: float32 [2, 32, 16, 64], P(None, 'tp'), may hold values from -0.75 to 0.75
- initial_state: float32 [2, 2, 32, 64], P(None, None, 'tp'), may hold values from -5 to 5
- intervals: float32 [1024], P('sp'), as said below
- proj_conv: bfloat16 [512, 2048], P('tp'), may hold values from -0.1875 to 0.1875
- proj_state: bfloat16 [512, 2048], P('tp'), may hold values from -0.1875 to 0.1875
Outputs:
- mixed: bfloat16 [1024, 2048], P('sp', 'tp')
The draws below stay inside these ranges and needn't reach their ends.
Inputs may be any that keep to these rules, and one draw needn't show every extreme that they name: `decay_rate`: Positive. `intervals`: Positive.
All inputs are finite; a program needn't handle non-finite values.
Results may differ from the reference program's by a relative error of at most 0.024.
Values may be sent and summed in bfloat16 or wider, within the bound.
A program may use at most 64 MiB of HBM per device.

```python
import math
import jax
import jax.numpy as jnp
from jax import lax

D = 2048
CONV_W = 512
SSM_W = 512
GSIZE = 16
STATE = 64
MIXER_GROUPS = 32
TOK_DEV = 128
TOKEN_COUNT = 1024
N_TP = 4


def rate_table(key):
    slow_share = 0.5
    slow_flags = jax.random.uniform(jax.random.fold_in(key, 101), (2, MIXER_GROUPS, 1)) < slow_share
    quantile = jax.random.uniform(jax.random.fold_in(key, 102), (2, MIXER_GROUPS, STATE))
    slow_rates = jnp.exp(math.log(0.4) + quantile * math.log(0.9 / 0.4)) / TOKEN_COUNT
    fast_rates = jnp.exp(math.log(0.01) + quantile * math.log(1.0 / 30.0 / 0.01))
    return jnp.where(slow_flags, slow_rates, fast_rates).astype(jnp.float32)


def driven_matrix(key, salt):
    decay_rates = rate_table(key)
    normal_part = jnp.clip(jax.random.normal(jax.random.fold_in(key, salt), (2, MIXER_GROUPS, STATE, GSIZE)), -5.0, 5.0)
    return (normal_part * jnp.sqrt(decay_rates / GSIZE)[..., None]).astype(jnp.float32)


def draw_decay_rate(key, part):
    return rate_table(key)


def draw_input_real(key, part):
    return driven_matrix(key, 103)


def draw_input_imag(key, part):
    return driven_matrix(key, 104)


def draw_intervals(key, part):
    blocks = TOKEN_COUNT // TOK_DEV
    factor = jnp.exp(jax.random.uniform(jax.random.fold_in(key, 1), (blocks, 1), minval=math.log(0.5), maxval=math.log(2.0)))
    jitter = jax.random.uniform(jax.random.fold_in(key, 2), (blocks, TOK_DEV), minval=0.5, maxval=1.5)
    evenly_spaced = (factor * jitter).reshape(TOKEN_COUNT)
    spike_locations = jax.random.randint(jax.random.fold_in(key, 3), (2,), 0, TOKEN_COUNT)
    slot_indices = jnp.arange(TOKEN_COUNT)
    spike_mask = (slot_indices == spike_locations[0]) | (slot_indices == spike_locations[1])
    return jnp.where(spike_mask, 0.5 * TOKEN_COUNT, evenly_spaced).astype(jnp.float32)


def draw_stream(key, part):
    normal_part = jnp.clip(jax.random.normal(jax.random.fold_in(key, 11), (TOKEN_COUNT, D)), -5.0, 5.0)
    rise = 3.0
    row_scale = jnp.exp(jax.random.uniform(jax.random.fold_in(key, 12), (TOKEN_COUNT, 1), minval=math.log(0.3), maxval=math.log(3.0)))
    column_scale = jnp.exp(jax.random.uniform(jax.random.fold_in(key, 13), (1, D), minval=math.log(0.5), maxval=math.log(1.6)))
    column_block = (jnp.arange(D) // (D // N_TP)).astype(jnp.float32)
    trend = rise ** (column_block / max(N_TP - 1, 1))
    return (normal_part * row_scale * column_scale * trend[None, :]).astype(jnp.bfloat16)


def steps_of(key, extent, split, least, top_value):
    gain, own = 1.0, jax.random.fold_in(key, 6)
    for axis_at, parts in split:
        steps = jnp.exp(jax.random.uniform(jax.random.fold_in(own, axis_at), (parts,), jnp.float32, least / len(split), top_value / len(split)))
        gain = gain * jnp.repeat(steps, extent[axis_at] // parts).reshape([-1 if axis == axis_at else 1 for axis in range(len(extent))])
    return gain


def noise(key, shape, deviation, most, shards=(), held_as=jnp.bfloat16):
    loudness = steps_of(key, shape, shards, -0.22, 0.18) if shards else 1.0
    drawn = jax.random.normal(key, shape, jnp.float32) * deviation * loudness
    return jnp.minimum(jnp.maximum(drawn, -most), most).astype(held_as)


def setup_inputs(seed: int = 0) -> dict:
    keys = jax.random.split(jax.random.key(seed), 19)
    return {
        "stream": draw_stream(jax.random.fold_in(keys[18], 71), 0),
        "norm_gain": jnp.clip(1.0 + 0.18 * jax.random.normal(keys[1], (D,), jnp.float32), 0.1, 1.9),
        "w_value": noise(keys[2], (D, CONV_W), D ** -0.5, 0.125, ((1, 4),)),
        "w_mix": noise(keys[3], (D, CONV_W), D ** -0.5, 0.125, ((1, 4),)),
        "w_gate": noise(keys[4], (D, CONV_W), D ** -0.5, 0.125, ((1, 4),)),
        "w_state": noise(keys[5], (D, SSM_W), D ** -0.5, 0.125, ((1, 4),)),
        "conv_taps": noise(keys[6], (3, CONV_W), 0.5, 3.0, ((1, 4),), jnp.float32),
        "skip_gain": noise(keys[7], (SSM_W,), 0.5, 3.0, ((0, 4),), jnp.float32),
        "decay_rate": draw_decay_rate(jax.random.fold_in(keys[18], 71), 0),
        "turn_rate": jnp.clip(0.25 + 1.25 * jax.random.uniform(keys[9], (2, MIXER_GROUPS, STATE), jnp.float32) ** steps_of(keys[9], (2, MIXER_GROUPS, STATE), ((1, 4),), -0.2, 0.2), 0.25, 1.5),
        "input_real": draw_input_real(jax.random.fold_in(keys[18], 71), 0),
        "input_imag": draw_input_imag(jax.random.fold_in(keys[18], 71), 0),
        "read_real": noise(keys[12], (2, MIXER_GROUPS, GSIZE, STATE), STATE ** -0.5, 0.75, ((1, 4),), jnp.float32),
        "read_imag": noise(keys[13], (2, MIXER_GROUPS, GSIZE, STATE), STATE ** -0.5, 0.75, ((1, 4),), jnp.float32),
        "initial_state": noise(keys[14], (2, 2, MIXER_GROUPS, STATE), 1.0, 5.0, ((2, 4),), jnp.float32),
        "intervals": draw_intervals(jax.random.fold_in(keys[18], 71), 0),
        "proj_conv": noise(keys[16], (CONV_W, D), (CONV_W + SSM_W) ** -0.5, 0.1875, ((0, 4),)),
        "proj_state": noise(keys[17], (SSM_W, D), (CONV_W + SSM_W) ** -0.5, 0.1875, ((0, 4),)),
    }


EPSILON = 1e-06
HIGH = lax.Precision.HIGHEST

def step_factors(decay_rate, turn_rate, interval):
    damping = -decay_rate * interval
    angle = turn_rate * interval
    magnitude = jnp.exp(damping)
    factor_re = magnitude * jnp.cos(angle)
    factor_im = magnitude * jnp.sin(angle)
    half_sine = jnp.sin(0.5 * angle)
    lift_re = jnp.expm1(damping) * jnp.cos(angle) - 2.0 * half_sine * half_sine
    denominator = decay_rate * decay_rate + turn_rate * turn_rate
    gain_real = (turn_rate * factor_im - decay_rate * lift_re) / denominator
    gain_im = -(decay_rate * factor_im + turn_rate * lift_re) / denominator
    return (factor_re, factor_im, gain_real, gain_im)

def state_direction(inputs, intervals, decay_rate, turn_rate, input_real, input_imag, read_real, read_imag, start_re, start_im, backward):
    block_count = TOKEN_COUNT // TOK_DEV
    input_blocks = inputs.reshape(block_count, TOK_DEV, MIXER_GROUPS, GSIZE)
    interval_blocks = intervals.reshape(block_count, TOK_DEV)

    def advance_block(boundary, block_items):
        block_inputs, block_steps = block_items
        factor_re, factor_im, gain_real, gain_im = step_factors(decay_rate, turn_rate, block_steps[:, None, None])
        driven_re = jnp.einsum('tgh,gph->tgp', block_inputs, input_real, precision=HIGH)
        driven_im = jnp.einsum('tgh,gph->tgp', block_inputs, input_imag, precision=HIGH)
        push_re = gain_real * driven_re - gain_im * driven_im
        push_im = gain_real * driven_im + gain_im * driven_re

        def advance_position(current, step_items):
            step_re, step_im, add_re, add_im = step_items
            new_re = step_re * current[0] - step_im * current[1] + add_re
            new_im = step_re * current[1] + step_im * current[0] + add_im
            return ((new_re, new_im), (new_re, new_im))
        boundary, history = lax.scan(advance_position, boundary, (factor_re, factor_im, push_re, push_im), reverse=backward)
        reading = jnp.einsum('ghp,tgp->tgh', read_real, history[0], precision=HIGH)
        reading = reading - jnp.einsum('ghp,tgp->tgh', read_imag, history[1], precision=HIGH)
        return (boundary, reading)
    _, readings = lax.scan(advance_block, (start_re, start_im), (input_blocks, interval_blocks), reverse=backward)
    return readings.reshape(TOKEN_COUNT, MIXER_GROUPS, GSIZE)

def reference(stream, norm_gain, w_value, w_mix, w_gate, w_state, conv_taps, skip_gain, decay_rate, turn_rate, input_real, input_imag, read_real, read_imag, initial_state, intervals, proj_conv, proj_state):
    widened = stream.astype(jnp.float32)
    inv_rms = lax.rsqrt(lax.optimization_barrier(jnp.mean(widened * widened, axis=1, keepdims=True)) + EPSILON)
    normed = (widened * inv_rms * norm_gain).astype(jnp.bfloat16)
    conv_value = jnp.dot(normed, w_value, preferred_element_type=jnp.float32).astype(jnp.bfloat16)
    conv_mix = jnp.dot(normed, w_mix, preferred_element_type=jnp.float32).astype(jnp.bfloat16)
    conv_gate = jnp.dot(normed, w_gate, preferred_element_type=jnp.float32).astype(jnp.bfloat16)
    state_input = jnp.dot(normed, w_state, preferred_element_type=jnp.float32).astype(jnp.bfloat16)
    source = (conv_mix.astype(jnp.float32) * conv_value.astype(jnp.float32)).astype(jnp.bfloat16)
    padded = jnp.pad(source.astype(jnp.float32), ((1, 1), (0, 0)))
    filtered = conv_taps[0] * padded[:-2] + conv_taps[1] * padded[1:-1] + conv_taps[2] * padded[2:]
    conv_out = (conv_gate.astype(jnp.float32) * filtered).astype(jnp.bfloat16)
    state_float = state_input.astype(jnp.float32).reshape(TOKEN_COUNT, MIXER_GROUPS, GSIZE)
    responses = skip_gain.reshape(MIXER_GROUPS, GSIZE) * state_float
    for direction in range(2):
        responses = responses + state_direction(state_float, intervals, decay_rate[direction], turn_rate[direction], input_real[direction], input_imag[direction], read_real[direction], read_imag[direction], initial_state[direction, 0], initial_state[direction, 1], direction == 1)
    state_out = jax.nn.gelu(responses.reshape(TOKEN_COUNT, SSM_W)).astype(jnp.bfloat16)
    total = jnp.dot(conv_out, proj_conv, preferred_element_type=jnp.float32)
    total = total + jnp.dot(state_out, proj_state, preferred_element_type=jnp.float32)
    return total.astype(jnp.bfloat16)
```

```python
import functools

import jax
import jax.numpy as jnp
from jax import lax
from jax.experimental import pallas as pl
from jax.experimental.pallas import tpu as pltpu
from jax.sharding import PartitionSpec as P

EPSILON = 1e-06
MESH = pl.DeviceIdType.MESH
F32 = jnp.float32
BF16 = jnp.bfloat16
CHUNKS = 2
OUT_CHUNKS = 2


def dot(a, b):
    return jnp.dot(a, b, preferred_element_type=F32)


def dot_t(a, b):
    return lax.dot_general(a, b, (((1,), (1,)), ((), ())), preferred_element_type=F32)


def half_turns(angle):
    theta = 0.5 * angle
    n = jnp.floor(theta * 0.6366197723675814 + 0.5)
    r = theta - n * 1.5703125
    r = r - n * 0.00048351287841796875
    r = r - n * 3.1385570764541626e-07
    r = r - n * 6.077100627776710e-11
    odd = (n - 2.0 * jnp.floor(0.5 * n)) > 0.5
    z = r * r
    s = r + r * z * ((-1.9515295891e-4 * z + 8.3321608736e-3) * z - 1.6666654611e-1)
    c = 1.0 - 0.5 * z + z * z * (
        (2.443315711809948e-5 * z - 1.388731625493765e-3) * z + 4.166664568298827e-2
    )
    square = jnp.where(odd, c * c, s * s)
    double = 2.0 * s * c
    return square, jnp.where(odd, -double, double)


def expm1_of(x, e):
    p = 1.0 + x * (1.0 / 7.0)
    for k in (6.0, 5.0, 4.0, 3.0, 2.0):
        p = 1.0 + x * p * (1.0 / k)
    return jnp.where(x > -0.35, x * p, e - 1.0)


def repeat(lo, hi, body):
    if hi - lo <= 16:
        for i in range(lo, hi):
            body(i)
    else:
        def step(i, carry):
            body(i)
            return carry
        lax.fori_loop(lo, hi, step, 0)


def kernel(
    n_sp, n_tp,
    x_ref, gain_ref, wv, wm, wg, ws, taps_ref, skip_ref, decay_ref, turn_ref,
    inr, ini, rdr, rdi, init_ref, iv_s, iv_ref, pc, ps,
    out_ref,
    w_all, p_all, in_v, rd_v, x_full, gains, el_all, fr_ref, fi_ref, gr_ref, gi_ref,
    dr_ref, di_ref, h0r, h0i, h1r, h1i, bt_ref, rt_ref, src_ref, halo_ref, e_out, e_all,
    blk_r, blk_i, p1_out, p1_in, p2_out, p2_in, c_out, c_in,
    load_sem, as_sem, ar_sem, bs_sem, br_sem, fs_sem, fwr_sem, gs_sem, grv_sem,
    is_sem, ir_sem, hs_sem, hr_sem, es_sem, er_sem, p1s, p1r, p2s, p2r, cs, cr,
):
    tp, sp = lax.axis_index("tp"), lax.axis_index("sp")
    rows, width = x_ref.shape
    channels = wv.shape[1]
    y, core = tp // 2, tp % 2
    sib = y * 2 + 1 - core
    oth = (1 - y) * 2 + core
    diag = (1 - y) * 2 + 1 - core
    cw = width // CHUNKS

    loads = []

    def load(src, dst):
        copy = pltpu.make_async_copy(src, dst, load_sem.at[len(loads)])
        copy.start()
        loads.append(copy)

    load(inr, in_v.at[0])
    load(ini, in_v.at[1])
    load(rdr, rd_v.at[0])
    load(rdi, rd_v.at[1])
    for j, w in enumerate((wv, wm, wg, ws)):
        load(w, w_all.at[:, pl.ds(j * channels, channels)])
    load(pc, p_all.at[pl.ds(0, channels)])
    load(ps, p_all.at[pl.ds(channels, channels)])

    barrier = pltpu.get_barrier_semaphore()
    for j in range(1, n_tp):
        pl.semaphore_signal(barrier, inc=1, device_id={"tp": (tp + j) % n_tp}, device_id_type=MESH)
    repeat(1, n_sp, lambda r: pl.semaphore_signal(
        barrier, inc=1, device_id={"sp": (sp + r) % n_sp}, device_id_type=MESH))
    pl.semaphore_wait(barrier, n_tp - 1 + n_sp - 1)

    def remote(src, dst, send, recv, where):
        return pltpu.make_async_remote_copy(
            src_ref=src, dst_ref=dst, send_sem=send, recv_sem=recv,
            device_id=where, device_id_type=MESH)

    to_sib, to_oth, forward = [], [], []
    for c in range(CHUNKS):
        piece = x_ref.at[:, pl.ds(c * cw, cw)]
        to_oth.append(remote(piece, x_full.at[tp, c], bs_sem.at[c], br_sem.at[c], {"tp": oth}))
        to_sib.append(remote(piece, x_full.at[tp, c], as_sem.at[c], ar_sem.at[c], {"tp": sib}))
        forward.append(remote(x_full.at[oth, c], x_full.at[oth, c], fs_sem.at[c], fwr_sem.at[c],
                              {"tp": sib}))
    gain_copies = [
        remote(gain_ref, gains.at[tp], gs_sem.at[j], grv_sem.at[j], {"tp": (tp + j) % n_tp})
        for j in range(1, n_tp)
    ]
    for copy in gain_copies:
        copy.start()
    for c in range(CHUNKS):
        to_oth[c].start()
        to_sib[c].start()

    def interval_copy(r):
        return remote(iv_ref, el_all.at[r], is_sem.at[r], ir_sem.at[r], {"sp": (sp + r) % n_sp})

    repeat(1, n_sp, lambda r: interval_copy(r).start())

    sub = lax.broadcasted_iota(jnp.int32, (8, 128), 0)
    top = sub < 4

    def pack(ref):
        even = ref[pl.ds(0, 8, stride=2), :]
        odd = ref[pl.ds(1, 8, stride=2), :]
        return jnp.concatenate([even, odd], axis=1)

    decay, turn = pack(decay_ref), pack(turn_ref)

    def pack_init(part):
        halves = [
            jnp.concatenate([init_ref[pl.ds(d * 16 + part * 8, 4, stride=2), :],
                             init_ref[pl.ds(d * 16 + part * 8 + 1, 4, stride=2), :]], axis=1)
            for d in range(2)
        ]
        return jnp.concatenate(halves, axis=0)

    init_r, init_i = pack_init(0), pack_init(1)
    den = decay * decay + turn * turn
    td, dd = turn / den, decay / den

    def factors(k, carry):
        iv = jnp.where(top, iv_s[k], iv_s[rows - 1 - k])
        damp = -decay * iv
        square, sine = half_turns(turn * iv)
        e = jnp.exp(damp)
        cosine = 1.0 - 2.0 * square
        f_im = e * sine
        lift = expm1_of(damp, e) * cosine - 2.0 * square
        at = pl.ds(pl.multiple_of(k * 8, 8), 8)
        fr_ref[at, :] = e * cosine
        fi_ref[at, :] = f_im
        gr_ref[at, :] = td * f_im - dd * lift
        gi_ref[at, :] = -(dd * f_im + td * lift)
        return carry

    lax.fori_loop(0, rows, factors, 0, unroll=4)

    for c in range(CHUNKS):
        to_oth[c].wait_recv()
        forward[c].start()

    for i in range(4):
        loads[i].wait()
    states = in_v.shape[1]
    group = in_v.shape[2]
    per = rd_v.shape[2]
    half = states // 2
    spread = (lax.broadcasted_iota(jnp.int32, (group, channels), 1) % group
              == lax.broadcasted_iota(jnp.int32, (group, channels), 0)).astype(BF16)
    keep = ((lax.broadcasted_iota(jnp.int32, (half, channels), 0) // per)
            == (lax.broadcasted_iota(jnp.int32, (half, channels), 1) // group))
    spread_r = (lax.broadcasted_iota(jnp.int32, (per, half), 1) % per
                == lax.broadcasted_iota(jnp.int32, (per, half), 0)).astype(BF16)
    keep_r = ((lax.broadcasted_iota(jnp.int32, (channels, half), 1) // per)
              == (lax.broadcasted_iota(jnp.int32, (channels, half), 0) // group))
    for part in range(2):
        for d in range(2):
            wide = dot(in_v[part, pl.ds(d * half, half), :].astype(BF16), spread)
            bt_ref[part, pl.ds(d * half, half), :] = jnp.where(keep, wide, 0.0).astype(BF16)
            wide = dot(rd_v[part, pl.ds(d * channels, channels), :].astype(BF16), spread_r)
            if part:
                wide = -wide
            rt_ref[part, :, pl.ds(d * half, half)] = jnp.where(keep_r, wide, 0.0).astype(BF16)

    for i in range(4, 8):
        loads[i].wait()
    for copy in gain_copies:
        copy.wait_recv()

    def project(value, gain, first):
        wide = value.astype(F32)
        scaled = (wide * gain).astype(BF16)
        term = dot(scaled, w_all[pl.ds(pl.multiple_of(first, cw), cw), :])
        return term, jnp.sum(wide * wide, axis=1, keepdims=True)

    projected = jnp.zeros((rows, 4 * channels), F32)
    squares = jnp.zeros((rows, 1), F32)
    for c in range(CHUNKS):
        t, s = project(x_ref[:, c * cw:(c + 1) * cw], gain_ref[:, c * cw:(c + 1) * cw],
                       tp * width + c * cw)
        projected, squares = projected + t, squares + s

    def remaining(owner, waits, projected, squares):
        for c in range(CHUNKS):
            if waits is not None:
                waits[c].wait_recv()
            t, s = project(x_full[owner, c], gains[owner][:, c * cw:(c + 1) * cw],
                           owner * width + c * cw)
            projected, squares = projected + t, squares + s
        return projected, squares

    projected, squares = remaining(sib, to_sib, projected, squares)
    projected, squares = remaining(oth, None, projected, squares)
    projected, squares = remaining(diag, forward, projected, squares)
    projected = projected * lax.rsqrt(squares / (width * n_tp) + EPSILON)
    conv_value = projected[:, :channels].astype(BF16).astype(F32)
    conv_mix = projected[:, channels:2 * channels].astype(BF16).astype(F32)
    conv_gate = projected[:, 2 * channels:3 * channels].astype(BF16).astype(F32)
    state_input = projected[:, 3 * channels:].astype(BF16)
    src_ref[...] = (conv_mix * conv_value).astype(BF16)

    for part, ref in ((0, dr_ref), (1, di_ref)):
        driven = dot_t(state_input, bt_ref[part])
        for j in range(8):
            ref[pl.ds(j, rows, stride=8), :] = driven[:, j * 128:(j + 1) * 128]

    halo_up = remote(src_ref.at[pl.ds(rows - 16, 16)], halo_ref.at[0], hs_sem.at[0], hr_sem.at[0],
                     {"sp": (sp + 1) % n_sp})
    halo_down = remote(src_ref.at[pl.ds(0, 16)], halo_ref.at[1], hs_sem.at[1], hr_sem.at[1],
                       {"sp": (sp + n_sp - 1) % n_sp})
    halo_up.start()
    halo_down.start()

    def first_pass(k, carry):
        hr, hi = carry
        at = pl.ds(pl.multiple_of(k * 8, 8), 8)
        back = pl.ds(pl.multiple_of((rows - 1 - k) * 8, 8), 8)
        dr = jnp.where(top, dr_ref[at, :], dr_ref[back, :])
        di = jnp.where(top, di_ref[at, :], di_ref[back, :])
        gr, gi = gr_ref[at, :], gi_ref[at, :]
        fr, fi = fr_ref[at, :], fi_ref[at, :]
        pr = gr * dr - gi * di
        pi = gr * di + gi * dr
        gr_ref[at, :] = pr
        gi_ref[at, :] = pi
        return fr * hr + (pr - fi * hi), fr * hi + (pi + fi * hr)

    zero = jnp.zeros((8, 128), F32)
    hr, hi = lax.fori_loop(0, rows, first_pass, (zero, zero), unroll=8)
    e_out[0] = hr
    e_out[1] = hi

    def edge_copy(r):
        return remote(e_out, e_all.at[r], es_sem.at[r], er_sem.at[r], {"sp": (sp + r) % n_sp})

    repeat(1, n_sp, lambda r: edge_copy(r).start())

    repeat(1, n_sp, lambda r: interval_copy(r).wait_recv())

    def block_factor(r):
        before = jnp.sum(el_all[r], axis=1, keepdims=True) * jnp.where(sp - r >= 0, 1.0, 0.0)
        after = jnp.sum(el_all[n_sp - r], axis=1, keepdims=True) * jnp.where(sp + r < n_sp, 1.0, 0.0)
        elapsed = jnp.where(top, before, after)
        square, sine = half_turns(turn * elapsed)
        e = jnp.exp(-decay * elapsed)
        blk_r[r] = e * (1.0 - 2.0 * square)
        blk_i[r] = e * sine

    repeat(1, n_sp, block_factor)

    halo_up.wait_recv()
    halo_down.wait_recv()
    source = src_ref[...].astype(F32)
    line = lax.broadcasted_iota(jnp.int32, (rows, channels), 0)
    before = halo_ref[0].astype(F32)[15:16, :] * jnp.where(sp > 0, 1.0, 0.0)
    after = halo_ref[1].astype(F32)[0:1, :] * jnp.where(sp < n_sp - 1, 1.0, 0.0)
    previous = jnp.where(line == 0, before, pltpu.roll(source, 1, 0))
    following = jnp.where(line == rows - 1, after, pltpu.roll(source, rows - 1, 0))
    filtered = taps_ref[0:1, :] * previous + taps_ref[1:2, :] * source + taps_ref[2:3, :] * following
    conv_out = (conv_gate * filtered).astype(BF16)
    for i in range(8, 10):
        loads[i].wait()

    repeat(1, n_sp, lambda r: edge_copy(r).wait_recv())

    def combine(r, hr, hi):
        er = jnp.where(top, jnp.where(sp - r >= 0, e_all[r, 0], 0.0),
                       jnp.where(sp + r < n_sp, e_all[n_sp - r, 0], 0.0))
        ei = jnp.where(top, jnp.where(sp - r >= 0, e_all[r, 1], 0.0),
                       jnp.where(sp + r < n_sp, e_all[n_sp - r, 1], 0.0))
        fr, fi = blk_r[r], blk_i[r]
        return fr * hr + (er - fi * hi), fr * hi + (ei + fi * hr)

    hr, hi = init_r, init_i
    if n_sp <= 16:
        for r in range(n_sp - 1, 0, -1):
            hr, hi = combine(r, hr, hi)
    else:
        hr, hi = lax.fori_loop(1, n_sp, lambda i, h: combine(n_sp - i, *h), (hr, hi))

    def second_pass(k, carry):
        hr, hi = carry
        at = pl.ds(pl.multiple_of(k * 8, 8), 8)
        back = pl.ds(pl.multiple_of((rows - 1 - k) * 8, 8), 8)
        fr, fi = fr_ref[at, :], fi_ref[at, :]
        nr = fr * hr + (gr_ref[at, :] - fi * hi)
        ni = fr * hi + (gi_ref[at, :] + fi * hr)
        h0r[at, :] = nr
        h0i[at, :] = ni
        h1r[back, :] = nr
        h1i[back, :] = ni
        return nr, ni

    lax.fori_loop(0, rows, second_pass, (hr, hi), unroll=8)

    response = state_input.astype(F32) * skip_ref[...]
    for part, (forth, back) in enumerate(((h0r, h1r), (h0i, h1i))):
        history = jnp.concatenate(
            [(forth if j < 4 else back)[pl.ds(j, rows, stride=8), :].astype(BF16) for j in range(8)],
            axis=1)
        response = response + dot_t(history, rt_ref[part])
    inner = 0.7978845608028654 * (response + 0.044715 * (response * response * response))
    state_out = (0.5 * response * (1.0 + jnp.tanh(inner))).astype(BF16)
    branches = jnp.concatenate([conv_out, state_out], axis=1)

    ow = width // OUT_CHUNKS

    def partial(owner, c):
        return dot(branches, p_all[:, pl.ds(pl.multiple_of(owner * width + c * ow, ow), ow)])

    first, second, cross = [], [], []
    for c in range(OUT_CHUNKS):
        p1_out[c] = partial(diag, c).astype(BF16)
        first.append(remote(p1_out.at[c], p1_in.at[c], p1s.at[c], p1r.at[c], {"tp": sib}))
        first[c].start()
    kept = [partial(oth, c) for c in range(OUT_CHUNKS)]
    for c in range(OUT_CHUNKS):
        first[c].wait_recv()
        c_out[c] = (kept[c] + p1_in[c].astype(F32)).astype(BF16)
        cross.append(remote(c_out.at[c], c_in.at[c], cs.at[c], cr.at[c], {"tp": oth}))
        cross[c].start()
    for c in range(OUT_CHUNKS):
        p2_out[c] = partial(sib, c).astype(BF16)
        second.append(remote(p2_out.at[c], p2_in.at[c], p2s.at[c], p2r.at[c], {"tp": sib}))
        second[c].start()
    mine = [partial(tp, c) for c in range(OUT_CHUNKS)]
    for c in range(OUT_CHUNKS):
        second[c].wait_recv()
        mine[c] = mine[c] + p2_in[c].astype(F32)
    for c in range(OUT_CHUNKS):
        cross[c].wait_recv()
        out_ref[:, c * ow:(c + 1) * ow] = (mine[c] + c_in[c].astype(F32)).astype(BF16)

    for copy in to_sib + to_oth + forward + gain_copies + [halo_up, halo_down] + first + second + cross:
        copy.wait_send()
    repeat(1, n_sp, lambda r: interval_copy(r).wait_send())
    repeat(1, n_sp, lambda r: edge_copy(r).wait_send())


def per_device(
    n_sp, n_tp,
    stream, norm_gain, w_value, w_mix, w_gate, w_state, conv_taps, skip_gain, decay_rate, turn_rate,
    input_real, input_imag, read_real, read_imag, initial_state, intervals, proj_conv, proj_state,
):
    rows, width = stream.shape
    channels = w_value.shape[1]
    dirs, groups, per, group = input_real.shape
    states = dirs * groups * per
    cw, ow = width // CHUNKS, width // OUT_CHUNKS
    vmem = pl.BlockSpec(memory_space=pltpu.VMEM)
    hbm = pl.BlockSpec(memory_space=pl.ANY)
    smem = pl.BlockSpec(memory_space=pltpu.SMEM)
    dma = lambda n: pltpu.SemaphoreType.DMA((n,))
    packed = pltpu.VMEM((rows * 8, 128), F32)
    return pl.pallas_call(
        functools.partial(kernel, n_sp, n_tp),
        out_shape=jax.ShapeDtypeStruct((rows, width), BF16),
        in_specs=[vmem, vmem, hbm, hbm, hbm, hbm, vmem, vmem, vmem, vmem,
                  hbm, hbm, hbm, hbm, vmem, smem, vmem, hbm, hbm],
        out_specs=vmem,
        scratch_shapes=[
            pltpu.VMEM((width * n_tp, 4 * channels), BF16),
            pltpu.VMEM((2 * channels, width * n_tp), BF16),
            pltpu.VMEM((2, states, group), F32),
            pltpu.VMEM((2, dirs * groups * group, per), F32),
            pltpu.VMEM((n_tp, CHUNKS, rows, cw), BF16),
            pltpu.VMEM((n_tp, 1, width), F32),
            pltpu.VMEM((n_sp, 1, rows), F32),
            packed, packed, packed, packed, packed, packed, packed, packed, packed, packed,
            pltpu.VMEM((2, states, channels), BF16),
            pltpu.VMEM((2, channels, states), BF16),
            pltpu.VMEM((rows, channels), BF16),
            pltpu.VMEM((2, 16, channels), BF16),
            pltpu.VMEM((2, 8, 128), F32),
            pltpu.VMEM((n_sp, 2, 8, 128), F32),
            pltpu.VMEM((n_sp, 8, 128), F32),
            pltpu.VMEM((n_sp, 8, 128), F32),
        ] + [pltpu.VMEM((OUT_CHUNKS, rows, ow), BF16)] * 6 + [
            dma(10),
            dma(CHUNKS), dma(CHUNKS), dma(CHUNKS), dma(CHUNKS), dma(CHUNKS), dma(CHUNKS),
            dma(n_tp), dma(n_tp), dma(n_sp), dma(n_sp), dma(2), dma(2), dma(n_sp), dma(n_sp),
            dma(OUT_CHUNKS), dma(OUT_CHUNKS), dma(OUT_CHUNKS), dma(OUT_CHUNKS),
            dma(OUT_CHUNKS), dma(OUT_CHUNKS),
        ],
        compiler_params=pltpu.CompilerParams(
            collective_id=0, has_side_effects=True, vmem_limit_bytes=48 * 1024 * 1024),
    )(
        stream, norm_gain.reshape(1, width), w_value, w_mix, w_gate, w_state, conv_taps,
        skip_gain.reshape(1, channels),
        decay_rate.reshape(dirs * groups, per), turn_rate.reshape(dirs * groups, per),
        input_real.reshape(states, group), input_imag.reshape(states, group),
        read_real.reshape(dirs * groups * group, per), read_imag.reshape(dirs * groups * group, per),
        initial_state.reshape(dirs * 2 * groups, per), intervals, intervals.reshape(1, rows),
        proj_conv, proj_state,
    )


def solution(mesh):
    return jax.shard_map(
        functools.partial(per_device, mesh.shape["sp"], mesh.shape["tp"]),
        mesh=mesh,
        in_specs=(
            P("sp", "tp"), P("tp"), P(None, "tp"), P(None, "tp"), P(None, "tp"), P(None, "tp"),
            P(None, "tp"), P("tp"), P(None, "tp", None), P(None, "tp", None),
            P(None, "tp", None, None), P(None, "tp", None, None), P(None, "tp", None, None),
            P(None, "tp", None, None), P(None, None, "tp", None), P("sp"), P("tp", None),
            P("tp", None),
        ),
        out_specs=P("sp", "tp"),
        check_vma=False,
    )
```

```python
import functools

import jax
import jax.numpy as jnp
from jax import lax
from jax.experimental import pallas as pl
from jax.experimental.pallas import tpu as pltpu
from jax.sharding import PartitionSpec as P

EPSILON = 1e-06
MESH = pl.DeviceIdType.MESH
F32 = jnp.float32
BF16 = jnp.bfloat16
CHUNKS = 2
OUT_CHUNKS = 2


def dot(a, b):
    return jnp.dot(a, b, preferred_element_type=F32)


def dot_t(a, b):
    return lax.dot_general(a, b, (((1,), (1,)), ((), ())), preferred_element_type=F32)


def half_turns(angle):
    theta = 0.5 * angle
    n = jnp.floor(theta * 0.6366197723675814 + 0.5)
    r = theta - n * 1.5703125
    r = r - n * 0.00048351287841796875
    r = r - n * 3.1385570764541626e-07
    r = r - n * 6.077100627776710e-11
    odd = (n - 2.0 * jnp.floor(0.5 * n)) > 0.5
    z = r * r
    s = r + r * z * ((-1.9515295891e-4 * z + 8.3321608736e-3) * z - 1.6666654611e-1)
    c = 1.0 - 0.5 * z + z * z * (
        (2.443315711809948e-5 * z - 1.388731625493765e-3) * z + 4.166664568298827e-2
    )
    square = jnp.where(odd, c * c, s * s)
    double = 2.0 * s * c
    return square, jnp.where(odd, -double, double)


def expm1_of(x, e):
    p = 1.0 + x * (1.0 / 7.0)
    for k in (6.0, 5.0, 4.0, 3.0, 2.0):
        p = 1.0 + x * p * (1.0 / k)
    return jnp.where(x > -0.35, x * p, e - 1.0)


def repeat(lo, hi, body):
    if hi - lo <= 16:
        for i in range(lo, hi):
            body(i)
    else:
        def step(i, carry):
            body(i)
            return carry
        lax.fori_loop(lo, hi, step, 0)


def kernel(
    n_sp, n_tp,
    x_hbm, gain_hbm, wv, wm, wg, ws, taps_hbm, skip_hbm, decay_hbm, turn_hbm,
    inr, ini, rdr, rdi, init_hbm, iv_hbm, pc, ps,
    out_ref,
    x_ref, gain_ref, taps_ref, skip_ref, decay_ref, turn_ref, init_ref, iv_s,
    w_all, p_all, in_v, rd_v, x_full, gains, el_all, fr_ref, fi_ref, gr_ref, gi_ref,
    dr_ref, di_ref, h0r, h0i, h1r, h1i, bt_ref, rt_ref, src_ref, halo_ref, e_out, e_all,
    blk_r, blk_i, p1_out, p1_in, p2_out, p2_in, c_out, c_in,
    load_sem, as_sem, ar_sem, bs_sem, br_sem, fs_sem, fwr_sem, gs_sem, grv_sem,
    is_sem, ir_sem, hs_sem, hr_sem, es_sem, er_sem, p1s, p1r, p2s, p2r, cs, cr,
):
    tp, sp = lax.axis_index("tp"), lax.axis_index("sp")
    rows, width = x_hbm.shape
    channels = wv.shape[1]
    y, core = tp // 2, tp % 2
    sib = y * 2 + 1 - core
    oth = (1 - y) * 2 + core
    diag = (1 - y) * 2 + 1 - core
    cw = width // CHUNKS

    loads = []

    def load(src, dst):
        copy = pltpu.make_async_copy(src, dst, load_sem.at[len(loads)])
        copy.start()
        loads.append(copy)

    barrier = pltpu.get_barrier_semaphore()
    for j in range(1, n_tp):
        pl.semaphore_signal(barrier, inc=1, device_id={"tp": (tp + j) % n_tp}, device_id_type=MESH)
    repeat(1, n_sp, lambda r: pl.semaphore_signal(
        barrier, inc=1, device_id={"sp": (sp + r) % n_sp}, device_id_type=MESH))
    load(iv_hbm, iv_s)
    load(decay_hbm, decay_ref)
    load(turn_hbm, turn_ref)
    load(init_hbm, init_ref)
    load(inr, in_v.at[0])
    load(ini, in_v.at[1])
    load(rdr, rd_v.at[0])
    load(rdi, rd_v.at[1])
    load(x_hbm, x_ref)
    load(gain_hbm, gain_ref)
    for j, w in enumerate((wv, wm, wg, ws)):
        load(w, w_all.at[:, pl.ds(j * channels, channels)])
    load(taps_hbm, taps_ref)
    load(skip_hbm, skip_ref)
    load(pc, p_all.at[pl.ds(0, channels)])
    load(ps, p_all.at[pl.ds(channels, channels)])
    pl.semaphore_wait(barrier, n_tp - 1 + n_sp - 1)

    def remote(src, dst, send, recv, where):
        return pltpu.make_async_remote_copy(
            src_ref=src, dst_ref=dst, send_sem=send, recv_sem=recv,
            device_id=where, device_id_type=MESH)

    to_sib, to_oth, forward = [], [], []
    for c in range(CHUNKS):
        piece = x_hbm.at[:, pl.ds(c * cw, cw)]
        to_oth.append(remote(piece, x_full.at[tp, c], bs_sem.at[c], br_sem.at[c], {"tp": oth}))
        to_sib.append(remote(piece, x_full.at[tp, c], as_sem.at[c], ar_sem.at[c], {"tp": sib}))
        forward.append(remote(x_full.at[oth, c], x_full.at[oth, c], fs_sem.at[c], fwr_sem.at[c],
                              {"tp": sib}))
    gain_copies = [
        remote(gain_hbm, gains.at[tp], gs_sem.at[j], grv_sem.at[j], {"tp": (tp + j) % n_tp})
        for j in range(1, n_tp)
    ]
    for copy in gain_copies:
        copy.start()
    for c in range(CHUNKS):
        to_oth[c].start()
        to_sib[c].start()

    def interval_copy(r):
        return remote(iv_hbm, el_all.at[r], is_sem.at[r], ir_sem.at[r], {"sp": (sp + r) % n_sp})

    repeat(1, n_sp, lambda r: interval_copy(r).start())

    sub = lax.broadcasted_iota(jnp.int32, (8, 128), 0)
    top = sub < 4

    def pack(ref):
        even = ref[pl.ds(0, 8, stride=2), :]
        odd = ref[pl.ds(1, 8, stride=2), :]
        return jnp.concatenate([even, odd], axis=1)

    for i in range(4):
        loads[i].wait()
    decay, turn = pack(decay_ref), pack(turn_ref)

    def pack_init(part):
        halves = [
            jnp.concatenate([init_ref[pl.ds(d * 16 + part * 8, 4, stride=2), :],
                             init_ref[pl.ds(d * 16 + part * 8 + 1, 4, stride=2), :]], axis=1)
            for d in range(2)
        ]
        return jnp.concatenate(halves, axis=0)

    init_r, init_i = pack_init(0), pack_init(1)
    den = decay * decay + turn * turn
    td, dd = turn / den, decay / den

    def factors(k, carry):
        iv = jnp.where(top, iv_s[0, k], iv_s[0, rows - 1 - k])
        damp = -decay * iv
        square, sine = half_turns(turn * iv)
        e = jnp.exp(damp)
        cosine = 1.0 - 2.0 * square
        f_im = e * sine
        lift = expm1_of(damp, e) * cosine - 2.0 * square
        at = pl.ds(pl.multiple_of(k * 8, 8), 8)
        fr_ref[at, :] = e * cosine
        fi_ref[at, :] = f_im
        gr_ref[at, :] = td * f_im - dd * lift
        gi_ref[at, :] = -(dd * f_im + td * lift)
        return carry

    for c in range(CHUNKS):
        lax.fori_loop(c * rows // CHUNKS, (c + 1) * rows // CHUNKS, factors, 0, unroll=4)
        to_oth[c].wait_recv()
        forward[c].start()

    for i in range(4, 8):
        loads[i].wait()
    states = bt_ref.shape[2]
    per = rd_v.shape[2]
    half = states // 2
    group = channels * per // half
    spread = (lax.broadcasted_iota(jnp.int32, (per, half), 1) % per
              == lax.broadcasted_iota(jnp.int32, (per, half), 0)).astype(BF16)
    keep = ((lax.broadcasted_iota(jnp.int32, (channels, half), 1) // per)
            == (lax.broadcasted_iota(jnp.int32, (channels, half), 0) // group))
    for part in range(2):
        for d in range(2):
            at, to = pl.ds(d * channels, channels), pl.ds(d * half, half)
            wide = dot(in_v[part, at, :].astype(BF16), spread)
            bt_ref[part, :, to] = jnp.where(keep, wide, 0.0).astype(BF16)
            wide = dot(rd_v[part, at, :].astype(BF16), spread)
            if part:
                wide = -wide
            rt_ref[part, :, to] = jnp.where(keep, wide, 0.0).astype(BF16)

    for i in range(8, 14):
        loads[i].wait()
    for copy in gain_copies:
        copy.wait_recv()

    def project(value, gain, first):
        wide = value.astype(F32)
        scaled = (wide * gain).astype(BF16)
        term = dot(scaled, w_all[pl.ds(pl.multiple_of(first, cw), cw), :])
        return term, jnp.sum(wide * wide, axis=1, keepdims=True)

    projected = jnp.zeros((rows, 4 * channels), F32)
    squares = jnp.zeros((rows, 1), F32)
    for c in range(CHUNKS):
        t, s = project(x_ref[:, c * cw:(c + 1) * cw], gain_ref[:, c * cw:(c + 1) * cw],
                       tp * width + c * cw)
        projected, squares = projected + t, squares + s

    def remaining(owner, waits, projected, squares):
        for c in range(CHUNKS):
            if waits is not None:
                waits[c].wait_recv()
            t, s = project(x_full[owner, c], gains[owner][:, c * cw:(c + 1) * cw],
                           owner * width + c * cw)
            projected, squares = projected + t, squares + s
        return projected, squares

    projected, squares = remaining(sib, to_sib, projected, squares)
    projected, squares = remaining(oth, None, projected, squares)
    projected, squares = remaining(diag, forward, projected, squares)
    projected = projected * lax.rsqrt(squares / (width * n_tp) + EPSILON)
    conv_value = projected[:, :channels].astype(BF16).astype(F32)
    conv_mix = projected[:, channels:2 * channels].astype(BF16).astype(F32)
    conv_gate = projected[:, 2 * channels:3 * channels].astype(BF16).astype(F32)
    state_input = projected[:, 3 * channels:].astype(BF16)
    src_ref[...] = (conv_mix * conv_value).astype(BF16)

    for part, ref in ((0, dr_ref), (1, di_ref)):
        driven = dot(state_input, bt_ref[part])
        for j in range(8):
            ref[pl.ds(j, rows, stride=8), :] = driven[:, j * 128:(j + 1) * 128]

    halo_up = remote(src_ref.at[pl.ds(rows - 16, 16)], halo_ref.at[0], hs_sem.at[0], hr_sem.at[0],
                     {"sp": (sp + 1) % n_sp})
    halo_down = remote(src_ref.at[pl.ds(0, 16)], halo_ref.at[1], hs_sem.at[1], hr_sem.at[1],
                       {"sp": (sp + n_sp - 1) % n_sp})
    halo_up.start()
    halo_down.start()

    def first_pass(k, carry):
        hr, hi = carry
        at = pl.ds(pl.multiple_of(k * 8, 8), 8)
        back = pl.ds(pl.multiple_of((rows - 1 - k) * 8, 8), 8)
        dr = jnp.where(top, dr_ref[at, :], dr_ref[back, :])
        di = jnp.where(top, di_ref[at, :], di_ref[back, :])
        gr, gi = gr_ref[at, :], gi_ref[at, :]
        fr, fi = fr_ref[at, :], fi_ref[at, :]
        pr = gr * dr - gi * di
        pi = gr * di + gi * dr
        gr_ref[at, :] = pr
        gi_ref[at, :] = pi
        return fr * hr + (pr - fi * hi), fr * hi + (pi + fi * hr)

    zero = jnp.zeros((8, 128), F32)
    hr, hi = lax.fori_loop(0, rows, first_pass, (zero, zero), unroll=8)
    e_out[0] = hr
    e_out[1] = hi

    def edge_copy(r):
        return remote(e_out, e_all.at[r], es_sem.at[r], er_sem.at[r], {"sp": (sp + r) % n_sp})

    repeat(1, n_sp, lambda r: edge_copy(r).start())

    repeat(1, n_sp, lambda r: interval_copy(r).wait_recv())

    def block_factor(r):
        before = jnp.sum(el_all[r], axis=1, keepdims=True) * jnp.where(sp - r >= 0, 1.0, 0.0)
        after = jnp.sum(el_all[n_sp - r], axis=1, keepdims=True) * jnp.where(sp + r < n_sp, 1.0, 0.0)
        elapsed = jnp.where(top, before, after)
        square, sine = half_turns(turn * elapsed)
        e = jnp.exp(-decay * elapsed)
        blk_r[r] = e * (1.0 - 2.0 * square)
        blk_i[r] = e * sine

    repeat(1, n_sp, block_factor)

    halo_up.wait_recv()
    halo_down.wait_recv()
    for i in range(14, 18):
        loads[i].wait()
    source = src_ref[...].astype(F32)
    line = lax.broadcasted_iota(jnp.int32, (rows, channels), 0)
    before = halo_ref[0].astype(F32)[15:16, :] * jnp.where(sp > 0, 1.0, 0.0)
    after = halo_ref[1].astype(F32)[0:1, :] * jnp.where(sp < n_sp - 1, 1.0, 0.0)
    previous = jnp.where(line == 0, before, pltpu.roll(source, 1, 0))
    following = jnp.where(line == rows - 1, after, pltpu.roll(source, rows - 1, 0))
    filtered = taps_ref[0:1, :] * previous + taps_ref[1:2, :] * source + taps_ref[2:3, :] * following
    conv_out = (conv_gate * filtered).astype(BF16)

    repeat(1, n_sp, lambda r: edge_copy(r).wait_recv())

    def combine(r, hr, hi):
        er = jnp.where(top, jnp.where(sp - r >= 0, e_all[r, 0], 0.0),
                       jnp.where(sp + r < n_sp, e_all[n_sp - r, 0], 0.0))
        ei = jnp.where(top, jnp.where(sp - r >= 0, e_all[r, 1], 0.0),
                       jnp.where(sp + r < n_sp, e_all[n_sp - r, 1], 0.0))
        fr, fi = blk_r[r], blk_i[r]
        return fr * hr + (er - fi * hi), fr * hi + (ei + fi * hr)

    hr, hi = init_r, init_i
    if n_sp <= 16:
        for r in range(n_sp - 1, 0, -1):
            hr, hi = combine(r, hr, hi)
    else:
        hr, hi = lax.fori_loop(1, n_sp, lambda i, h: combine(n_sp - i, *h), (hr, hi))

    def second_pass(k, carry):
        hr, hi = carry
        at = pl.ds(pl.multiple_of(k * 8, 8), 8)
        back = pl.ds(pl.multiple_of((rows - 1 - k) * 8, 8), 8)
        fr, fi = fr_ref[at, :], fi_ref[at, :]
        nr = fr * hr + (gr_ref[at, :] - fi * hi)
        ni = fr * hi + (gi_ref[at, :] + fi * hr)
        h0r[at, :] = nr
        h0i[at, :] = ni
        h1r[back, :] = nr
        h1i[back, :] = ni
        return nr, ni

    lax.fori_loop(0, rows, second_pass, (hr, hi), unroll=8)

    response = state_input.astype(F32) * skip_ref[...]
    for part, (forth, back) in enumerate(((h0r, h1r), (h0i, h1i))):
        history = jnp.concatenate(
            [(forth if j < 4 else back)[pl.ds(j, rows, stride=8), :].astype(BF16) for j in range(8)],
            axis=1)
        response = response + dot_t(history, rt_ref[part])
    inner = 0.7978845608028654 * (response + 0.044715 * (response * response * response))
    state_out = (0.5 * response * (1.0 + jnp.tanh(inner))).astype(BF16)
    branches = jnp.concatenate([conv_out, state_out], axis=1)

    ow = width // OUT_CHUNKS

    def partial(owner, c):
        return dot(branches, p_all[:, pl.ds(pl.multiple_of(owner * width + c * ow, ow), ow)])

    first, second, cross = [], [], []
    for c in range(OUT_CHUNKS):
        p1_out[c] = partial(diag, c).astype(BF16)
        first.append(remote(p1_out.at[c], p1_in.at[c], p1s.at[c], p1r.at[c], {"tp": sib}))
        first[c].start()
    kept = [partial(oth, c) for c in range(OUT_CHUNKS)]
    for c in range(OUT_CHUNKS):
        first[c].wait_recv()
        c_out[c] = (kept[c] + p1_in[c].astype(F32)).astype(BF16)
        cross.append(remote(c_out.at[c], c_in.at[c], cs.at[c], cr.at[c], {"tp": oth}))
        cross[c].start()
    for c in range(OUT_CHUNKS):
        p2_out[c] = partial(sib, c).astype(BF16)
        second.append(remote(p2_out.at[c], p2_in.at[c], p2s.at[c], p2r.at[c], {"tp": sib}))
        second[c].start()
    mine = [partial(tp, c) for c in range(OUT_CHUNKS)]
    for c in range(OUT_CHUNKS):
        second[c].wait_recv()
        mine[c] = mine[c] + p2_in[c].astype(F32)
    for c in range(OUT_CHUNKS):
        cross[c].wait_recv()
        out_ref[:, c * ow:(c + 1) * ow] = (mine[c] + c_in[c].astype(F32)).astype(BF16)

    for copy in to_sib + to_oth + forward + gain_copies + [halo_up, halo_down] + first + second + cross:
        copy.wait_send()
    repeat(1, n_sp, lambda r: interval_copy(r).wait_send())
    repeat(1, n_sp, lambda r: edge_copy(r).wait_send())


def per_device(
    n_sp, n_tp,
    stream, norm_gain, w_value, w_mix, w_gate, w_state, conv_taps, skip_gain, decay_rate, turn_rate,
    input_real, input_imag, read_real, read_imag, initial_state, intervals, proj_conv, proj_state,
):
    rows, width = stream.shape
    channels = w_value.shape[1]
    dirs, groups, per, group = input_real.shape
    states = dirs * groups * per
    cw, ow = width // CHUNKS, width // OUT_CHUNKS
    hbm = pl.BlockSpec(memory_space=pltpu.HBM)
    dma = lambda n: pltpu.SemaphoreType.DMA((n,))
    packed = pltpu.VMEM((rows * 8, 128), F32)
    rows_of = lambda m: jnp.swapaxes(m, 2, 3).reshape(dirs * groups * group, per)
    return pl.pallas_call(
        functools.partial(kernel, n_sp, n_tp),
        out_shape=jax.ShapeDtypeStruct((rows, width), BF16),
        in_specs=[hbm] * 18,
        out_specs=pl.BlockSpec(memory_space=pltpu.VMEM),
        scratch_shapes=[
            pltpu.VMEM((rows, width), BF16),
            pltpu.VMEM((1, width), F32),
            pltpu.VMEM(conv_taps.shape, F32),
            pltpu.VMEM((1, channels), F32),
            pltpu.VMEM((dirs * groups, per), F32),
            pltpu.VMEM((dirs * groups, per), F32),
            pltpu.VMEM((dirs * 2 * groups, per), F32),
            pltpu.SMEM((1, rows), F32),
            pltpu.VMEM((width * n_tp, 4 * channels), BF16),
            pltpu.VMEM((2 * channels, width * n_tp), BF16),
            pltpu.VMEM((2, dirs * groups * group, per), F32),
            pltpu.VMEM((2, dirs * groups * group, per), F32),
            pltpu.VMEM((n_tp, CHUNKS, rows, cw), BF16),
            pltpu.VMEM((n_tp, 1, width), F32),
            pltpu.VMEM((n_sp, 1, rows), F32),
            packed, packed, packed, packed, packed, packed, packed, packed, packed, packed,
            pltpu.VMEM((2, channels, states), BF16),
            pltpu.VMEM((2, channels, states), BF16),
            pltpu.VMEM((rows, channels), BF16),
            pltpu.VMEM((2, 16, channels), BF16),
            pltpu.VMEM((2, 8, 128), F32),
            pltpu.VMEM((n_sp, 2, 8, 128), F32),
            pltpu.VMEM((n_sp, 8, 128), F32),
            pltpu.VMEM((n_sp, 8, 128), F32),
        ] + [pltpu.VMEM((OUT_CHUNKS, rows, ow), BF16)] * 6 + [
            dma(18),
            dma(CHUNKS), dma(CHUNKS), dma(CHUNKS), dma(CHUNKS), dma(CHUNKS), dma(CHUNKS),
            dma(n_tp), dma(n_tp), dma(n_sp), dma(n_sp), dma(2), dma(2), dma(n_sp), dma(n_sp),
            dma(OUT_CHUNKS), dma(OUT_CHUNKS), dma(OUT_CHUNKS), dma(OUT_CHUNKS),
            dma(OUT_CHUNKS), dma(OUT_CHUNKS),
        ],
        compiler_params=pltpu.CompilerParams(
            collective_id=0, has_side_effects=True, vmem_limit_bytes=67043328),
    )(
        stream, norm_gain.reshape(1, width), w_value, w_mix, w_gate, w_state, conv_taps,
        skip_gain.reshape(1, channels),
        decay_rate.reshape(dirs * groups, per), turn_rate.reshape(dirs * groups, per),
        rows_of(input_real), rows_of(input_imag),
        read_real.reshape(dirs * groups * group, per), read_imag.reshape(dirs * groups * group, per),
        initial_state.reshape(dirs * 2 * groups, per), intervals.reshape(1, rows),
        proj_conv, proj_state,
    )


def solution(mesh):
    return jax.shard_map(
        functools.partial(per_device, mesh.shape["sp"], mesh.shape["tp"]),
        mesh=mesh,
        in_specs=(
            P("sp", "tp"), P("tp"), P(None, "tp"), P(None, "tp"), P(None, "tp"), P(None, "tp"),
            P(None, "tp"), P("tp"), P(None, "tp", None), P(None, "tp", None),
            P(None, "tp", None, None), P(None, "tp", None, None), P(None, "tp", None, None),
            P(None, "tp", None, None), P(None, None, "tp", None), P("sp"), P("tp", None),
            P("tp", None),
        ),
        out_specs=P("sp", "tp"),
        check_vma=False,
    )
```

```python
import functools

import jax
import jax.numpy as jnp
from jax import lax
from jax.experimental import pallas as pl
from jax.experimental.pallas import tpu as pltpu
from jax.sharding import PartitionSpec as P

EPSILON = 1e-06
MESH = pl.DeviceIdType.MESH
F32 = jnp.float32
BF16 = jnp.bfloat16
CHUNKS = 2
OUT_CHUNKS = 2


def dot(a, b):
    return jnp.dot(a, b, preferred_element_type=F32)


def dot_t(a, b):
    return lax.dot_general(a, b, (((1,), (1,)), ((), ())), preferred_element_type=F32)


def half_turns(angle):
    theta = 0.5 * angle
    n = jnp.floor(theta * 0.6366197723675814 + 0.5)
    r = theta - n * 1.5703125
    r = r - n * 0.00048351287841796875
    r = r - n * 3.1385570764541626e-07
    r = r - n * 6.077100627776710e-11
    odd = (n - 2.0 * jnp.floor(0.5 * n)) > 0.5
    z = r * r
    s = r + r * z * ((-1.9515295891e-4 * z + 8.3321608736e-3) * z - 1.6666654611e-1)
    c = 1.0 - 0.5 * z + z * z * (
        (2.443315711809948e-5 * z - 1.388731625493765e-3) * z + 4.166664568298827e-2
    )
    square = jnp.where(odd, c * c, s * s)
    double = 2.0 * s * c
    return square, jnp.where(odd, -double, double)


def expm1_of(x, e):
    p = 1.0 + x * (1.0 / 7.0)
    for k in (6.0, 5.0, 4.0, 3.0, 2.0):
        p = 1.0 + x * p * (1.0 / k)
    return jnp.where(x > -0.35, x * p, e - 1.0)


def repeat(lo, hi, body):
    if hi - lo <= 16:
        for i in range(lo, hi):
            body(i)
    else:
        def step(i, carry):
            body(i)
            return carry
        lax.fori_loop(lo, hi, step, 0)


def kernel(
    n_sp, n_tp,
    x_hbm, gain_hbm, wv, wm, wg, ws, taps_hbm, skip_hbm, decay_hbm, turn_hbm,
    inr, ini, rdr, rdi, init_hbm, iv_hbm, pc, ps,
    out_ref,
    x_ref, gain_ref, taps_ref, skip_ref, decay_ref, turn_ref, init_ref, iv_s,
    w_all, pc_all, ps_all, so_all, acc_ref, in_v, rd_v, x_full, gains, el_all, fr_ref, fi_ref, gr_ref, gi_ref,
    dr_ref, di_ref, h0r, h0i, h1r, h1i, bt_ref, rt_ref, src_ref, halo_ref, e_out, e_all,
    blk_r, blk_i, p1_out, p1_in, p2_out, p2_in, c_out, c_in,
    load_sem, as_sem, ar_sem, bs_sem, br_sem, fs_sem, fwr_sem, gs_sem, grv_sem,
    is_sem, ir_sem, hs_sem, hr_sem, es_sem, er_sem, p1s, p1r, p2s, p2r, cs, cr, ws_sem, wr_sem, os_sem, or_sem,
):
    tp, sp = lax.axis_index("tp"), lax.axis_index("sp")
    rows, width = x_hbm.shape
    channels = wv.shape[1]
    y, core = tp // 2, tp % 2
    sib = y * 2 + 1 - core
    oth = (1 - y) * 2 + core
    diag = (1 - y) * 2 + 1 - core
    cw = width // CHUNKS

    loads = []

    def load(src, dst):
        copy = pltpu.make_async_copy(src, dst, load_sem.at[len(loads)])
        copy.start()
        loads.append(copy)

    barrier = pltpu.get_barrier_semaphore()
    for j in range(1, n_tp):
        pl.semaphore_signal(barrier, inc=1, device_id={"tp": (tp + j) % n_tp}, device_id_type=MESH)
    repeat(1, n_sp, lambda r: pl.semaphore_signal(
        barrier, inc=1, device_id={"sp": (sp + r) % n_sp}, device_id_type=MESH))
    load(iv_hbm, iv_s)
    load(decay_hbm, decay_ref)
    load(turn_hbm, turn_ref)
    load(init_hbm, init_ref)
    load(inr, in_v.at[0])
    load(ini, in_v.at[1])
    load(rdr, rd_v.at[0])
    load(rdi, rd_v.at[1])
    load(x_hbm, x_ref)
    load(gain_hbm, gain_ref)
    for j, w in enumerate((wv, wm, wg, ws)):
        load(w, w_all.at[:, pl.ds(j * channels, channels)])
    load(taps_hbm, taps_ref)
    load(skip_hbm, skip_ref)
    load(pc, pc_all)
    load(ps.at[:, pl.ds(pl.multiple_of(tp * width, width), width)], ps_all.at[tp])
    pl.semaphore_wait(barrier, n_tp - 1 + n_sp - 1)

    def remote(src, dst, send, recv, where):
        return pltpu.make_async_remote_copy(
            src_ref=src, dst_ref=dst, send_sem=send, recv_sem=recv,
            device_id=where, device_id_type=MESH)

    to_sib, to_oth, forward = [], [], []
    for c in range(CHUNKS):
        piece = x_hbm.at[:, pl.ds(c * cw, cw)]
        to_oth.append(remote(piece, x_full.at[tp, c], bs_sem.at[c], br_sem.at[c], {"tp": oth}))
        to_sib.append(remote(piece, x_full.at[tp, c], as_sem.at[c], ar_sem.at[c], {"tp": sib}))
        forward.append(remote(x_full.at[oth, c], x_full.at[oth, c], fs_sem.at[c], fwr_sem.at[c],
                              {"tp": sib}))
    gain_copies = [
        remote(gain_hbm, gains.at[tp], gs_sem.at[j], grv_sem.at[j], {"tp": (tp + j) % n_tp})
        for j in range(1, n_tp)
    ]
    for copy in gain_copies:
        copy.start()
    for c in range(CHUNKS):
        to_oth[c].start()
        to_sib[c].start()

    weight_copies, state_copies = [], []
    for j in range(1, n_tp):
        peer = (tp + j) % n_tp
        weight_copies.append(remote(
            ps.at[:, pl.ds(pl.multiple_of(peer * width, width), width)], ps_all.at[tp],
            ws_sem.at[j], wr_sem.at[j], {"tp": peer}))
        weight_copies[-1].start()
        state_copies.append(remote(
            so_all.at[tp], so_all.at[tp], os_sem.at[j], or_sem.at[j], {"tp": peer}))

    def interval_copy(r):
        return remote(iv_hbm, el_all.at[r], is_sem.at[r], ir_sem.at[r], {"sp": (sp + r) % n_sp})

    repeat(1, n_sp, lambda r: interval_copy(r).start())

    sub = lax.broadcasted_iota(jnp.int32, (8, 128), 0)
    top = sub < 4

    def pack(ref):
        even = ref[pl.ds(0, 8, stride=2), :]
        odd = ref[pl.ds(1, 8, stride=2), :]
        return jnp.concatenate([even, odd], axis=1)

    for i in range(4):
        loads[i].wait()
    decay, turn = pack(decay_ref), pack(turn_ref)

    def pack_init(part):
        halves = [
            jnp.concatenate([init_ref[pl.ds(d * 16 + part * 8, 4, stride=2), :],
                             init_ref[pl.ds(d * 16 + part * 8 + 1, 4, stride=2), :]], axis=1)
            for d in range(2)
        ]
        return jnp.concatenate(halves, axis=0)

    init_r, init_i = pack_init(0), pack_init(1)
    den = decay * decay + turn * turn
    td, dd = turn / den, decay / den

    def factors(k, carry):
        iv = jnp.where(top, iv_s[0, k], iv_s[0, rows - 1 - k])
        damp = -decay * iv
        square, sine = half_turns(turn * iv)
        e = jnp.exp(damp)
        cosine = 1.0 - 2.0 * square
        f_im = e * sine
        lift = expm1_of(damp, e) * cosine - 2.0 * square
        at = pl.ds(pl.multiple_of(k * 8, 8), 8)
        fr_ref[at, :] = e * cosine
        fi_ref[at, :] = f_im
        gr_ref[at, :] = td * f_im - dd * lift
        gi_ref[at, :] = -(dd * f_im + td * lift)
        return carry

    for c in range(CHUNKS):
        lax.fori_loop(c * rows // CHUNKS, (c + 1) * rows // CHUNKS, factors, 0, unroll=4)
        to_oth[c].wait_recv()
        forward[c].start()

    for i in range(4, 8):
        loads[i].wait()
    states = bt_ref.shape[2]
    per = rd_v.shape[2]
    half = states // 2
    group = channels * per // half
    spread = (lax.broadcasted_iota(jnp.int32, (per, half), 1) % per
              == lax.broadcasted_iota(jnp.int32, (per, half), 0)).astype(BF16)
    keep = ((lax.broadcasted_iota(jnp.int32, (channels, half), 1) // per)
            == (lax.broadcasted_iota(jnp.int32, (channels, half), 0) // group))
    for part in range(2):
        for d in range(2):
            at, to = pl.ds(d * channels, channels), pl.ds(d * half, half)
            wide = dot(in_v[part, at, :].astype(BF16), spread)
            bt_ref[part, :, to] = jnp.where(keep, wide, 0.0).astype(BF16)
            wide = dot(rd_v[part, at, :].astype(BF16), spread)
            if part:
                wide = -wide
            rt_ref[part, :, to] = jnp.where(keep, wide, 0.0).astype(BF16)

    for i in range(8, 14):
        loads[i].wait()
    for copy in gain_copies:
        copy.wait_recv()

    def project(value, gain, first):
        wide = value.astype(F32)
        scaled = (wide * gain).astype(BF16)
        term = dot(scaled, w_all[pl.ds(pl.multiple_of(first, cw), cw), :])
        return term, jnp.sum(wide * wide, axis=1, keepdims=True)

    projected = jnp.zeros((rows, 4 * channels), F32)
    squares = jnp.zeros((rows, 1), F32)
    for c in range(CHUNKS):
        t, s = project(x_ref[:, c * cw:(c + 1) * cw], gain_ref[:, c * cw:(c + 1) * cw],
                       tp * width + c * cw)
        projected, squares = projected + t, squares + s

    def remaining(owner, waits, projected, squares):
        for c in range(CHUNKS):
            if waits is not None:
                waits[c].wait_recv()
            t, s = project(x_full[owner, c], gains[owner][:, c * cw:(c + 1) * cw],
                           owner * width + c * cw)
            projected, squares = projected + t, squares + s
        return projected, squares

    projected, squares = remaining(sib, to_sib, projected, squares)
    projected, squares = remaining(oth, None, projected, squares)
    projected, squares = remaining(diag, forward, projected, squares)
    projected = projected * lax.rsqrt(squares / (width * n_tp) + EPSILON)
    conv_value = projected[:, :channels].astype(BF16).astype(F32)
    conv_mix = projected[:, channels:2 * channels].astype(BF16).astype(F32)
    conv_gate = projected[:, 2 * channels:3 * channels].astype(BF16).astype(F32)
    state_input = projected[:, 3 * channels:].astype(BF16)
    src_ref[...] = (conv_mix * conv_value).astype(BF16)

    for part, ref in ((0, dr_ref), (1, di_ref)):
        driven = dot(state_input, bt_ref[part])
        for j in range(8):
            ref[pl.ds(j, rows, stride=8), :] = driven[:, j * 128:(j + 1) * 128]

    halo_up = remote(src_ref.at[pl.ds(rows - 16, 16)], halo_ref.at[0], hs_sem.at[0], hr_sem.at[0],
                     {"sp": (sp + 1) % n_sp})
    halo_down = remote(src_ref.at[pl.ds(0, 16)], halo_ref.at[1], hs_sem.at[1], hr_sem.at[1],
                       {"sp": (sp + n_sp - 1) % n_sp})
    halo_up.start()
    halo_down.start()

    def first_pass(k, carry):
        hr, hi = carry
        at = pl.ds(pl.multiple_of(k * 8, 8), 8)
        back = pl.ds(pl.multiple_of((rows - 1 - k) * 8, 8), 8)
        dr = jnp.where(top, dr_ref[at, :], dr_ref[back, :])
        di = jnp.where(top, di_ref[at, :], di_ref[back, :])
        gr, gi = gr_ref[at, :], gi_ref[at, :]
        fr, fi = fr_ref[at, :], fi_ref[at, :]
        pr = gr * dr - gi * di
        pi = gr * di + gi * dr
        gr_ref[at, :] = pr
        gi_ref[at, :] = pi
        return fr * hr + (pr - fi * hi), fr * hi + (pi + fi * hr)

    zero = jnp.zeros((8, 128), F32)
    hr, hi = lax.fori_loop(0, rows, first_pass, (zero, zero), unroll=8)
    e_out[0] = hr
    e_out[1] = hi

    def edge_copy(r):
        return remote(e_out, e_all.at[r], es_sem.at[r], er_sem.at[r], {"sp": (sp + r) % n_sp})

    repeat(1, n_sp, lambda r: edge_copy(r).start())

    repeat(1, n_sp, lambda r: interval_copy(r).wait_recv())

    def block_factor(r):
        before = jnp.sum(el_all[r], axis=1, keepdims=True) * jnp.where(sp - r >= 0, 1.0, 0.0)
        after = jnp.sum(el_all[n_sp - r], axis=1, keepdims=True) * jnp.where(sp + r < n_sp, 1.0, 0.0)
        elapsed = jnp.where(top, before, after)
        square, sine = half_turns(turn * elapsed)
        e = jnp.exp(-decay * elapsed)
        blk_r[r] = e * (1.0 - 2.0 * square)
        blk_i[r] = e * sine

    repeat(1, n_sp, block_factor)

    halo_up.wait_recv()
    halo_down.wait_recv()
    for i in range(14, 18):
        loads[i].wait()
    source = src_ref[...].astype(F32)
    line = lax.broadcasted_iota(jnp.int32, (rows, channels), 0)
    before = halo_ref[0].astype(F32)[15:16, :] * jnp.where(sp > 0, 1.0, 0.0)
    after = halo_ref[1].astype(F32)[0:1, :] * jnp.where(sp < n_sp - 1, 1.0, 0.0)
    previous = jnp.where(line == 0, before, pltpu.roll(source, 1, 0))
    following = jnp.where(line == rows - 1, after, pltpu.roll(source, rows - 1, 0))
    filtered = taps_ref[0:1, :] * previous + taps_ref[1:2, :] * source + taps_ref[2:3, :] * following
    conv_out = (conv_gate * filtered).astype(BF16)

    ow = width // OUT_CHUNKS

    def partial(owner, c):
        return dot(conv_out, pc_all[:, pl.ds(pl.multiple_of(owner * width + c * ow, ow), ow)])

    first, second, cross = [], [], []
    for c in range(OUT_CHUNKS):
        p1_out[c] = partial(diag, c).astype(BF16)
        first.append(remote(p1_out.at[c], p1_in.at[c], p1s.at[c], p1r.at[c], {"tp": sib}))
        first[c].start()
    for c in range(OUT_CHUNKS):
        p2_out[c] = partial(sib, c).astype(BF16)
        second.append(remote(p2_out.at[c], p2_in.at[c], p2s.at[c], p2r.at[c], {"tp": sib}))
        second[c].start()
    for c in range(OUT_CHUNKS):
        acc_ref[:, c * ow:(c + 1) * ow] = partial(tp, c)
    kept = [partial(oth, c) for c in range(OUT_CHUNKS)]
    for c in range(OUT_CHUNKS):
        first[c].wait_recv()
        c_out[c] = (kept[c] + p1_in[c].astype(F32)).astype(BF16)
        cross.append(remote(c_out.at[c], c_in.at[c], cs.at[c], cr.at[c], {"tp": oth}))
        cross[c].start()

    repeat(1, n_sp, lambda r: edge_copy(r).wait_recv())

    def combine(r, hr, hi):
        er = jnp.where(top, jnp.where(sp - r >= 0, e_all[r, 0], 0.0),
                       jnp.where(sp + r < n_sp, e_all[n_sp - r, 0], 0.0))
        ei = jnp.where(top, jnp.where(sp - r >= 0, e_all[r, 1], 0.0),
                       jnp.where(sp + r < n_sp, e_all[n_sp - r, 1], 0.0))
        fr, fi = blk_r[r], blk_i[r]
        return fr * hr + (er - fi * hi), fr * hi + (ei + fi * hr)

    hr, hi = init_r, init_i
    if n_sp <= 16:
        for r in range(n_sp - 1, 0, -1):
            hr, hi = combine(r, hr, hi)
    else:
        hr, hi = lax.fori_loop(1, n_sp, lambda i, h: combine(n_sp - i, *h), (hr, hi))

    def second_pass(k, carry):
        hr, hi = carry
        at = pl.ds(pl.multiple_of(k * 8, 8), 8)
        back = pl.ds(pl.multiple_of((rows - 1 - k) * 8, 8), 8)
        fr, fi = fr_ref[at, :], fi_ref[at, :]
        nr = fr * hr + (gr_ref[at, :] - fi * hi)
        ni = fr * hi + (gi_ref[at, :] + fi * hr)
        h0r[at, :] = nr
        h0i[at, :] = ni
        h1r[back, :] = nr
        h1i[back, :] = ni
        return nr, ni

    lax.fori_loop(0, rows, second_pass, (hr, hi), unroll=8)

    response = state_input.astype(F32) * skip_ref[...]
    for part, (forth, back) in enumerate(((h0r, h1r), (h0i, h1i))):
        history = jnp.concatenate(
            [(forth if j < 4 else back)[pl.ds(j, rows, stride=8), :].astype(BF16) for j in range(8)],
            axis=1)
        response = response + dot_t(history, rt_ref[part])
    inner = 0.7978845608028654 * (response + 0.044715 * (response * response * response))
    state_out = (0.5 * response * (1.0 + jnp.tanh(inner))).astype(BF16)

    so_all[tp] = state_out
    for copy in state_copies:
        copy.start()
    total = acc_ref[...]
    for c in range(OUT_CHUNKS):
        second[c].wait_recv()
    total = total + jnp.concatenate([p2_in[c].astype(F32) for c in range(OUT_CHUNKS)], axis=1)
    for copy in weight_copies:
        copy.wait_recv()
    total = total + dot(state_out, ps_all[tp])
    for c in range(OUT_CHUNKS):
        cross[c].wait_recv()
    total = total + jnp.concatenate([c_in[c].astype(F32) for c in range(OUT_CHUNKS)], axis=1)
    for j in range(1, n_tp):
        state_copies[j - 1].wait_recv()
        owner = (tp + n_tp - j) % n_tp
        total = total + dot(so_all[owner], ps_all[owner])
    out_ref[...] = total.astype(BF16)

    for copy in to_sib + to_oth + forward + gain_copies + [halo_up, halo_down] + first + second + cross + weight_copies + state_copies:
        copy.wait_send()
    repeat(1, n_sp, lambda r: interval_copy(r).wait_send())
    repeat(1, n_sp, lambda r: edge_copy(r).wait_send())


def per_device(
    n_sp, n_tp,
    stream, norm_gain, w_value, w_mix, w_gate, w_state, conv_taps, skip_gain, decay_rate, turn_rate,
    input_real, input_imag, read_real, read_imag, initial_state, intervals, proj_conv, proj_state,
):
    rows, width = stream.shape
    channels = w_value.shape[1]
    dirs, groups, per, group = input_real.shape
    states = dirs * groups * per
    cw, ow = width // CHUNKS, width // OUT_CHUNKS
    hbm = pl.BlockSpec(memory_space=pltpu.HBM)
    dma = lambda n: pltpu.SemaphoreType.DMA((n,))
    packed = pltpu.VMEM((rows * 8, 128), F32)
    rows_of = lambda m: jnp.swapaxes(m, 2, 3).reshape(dirs * groups * group, per)
    return pl.pallas_call(
        functools.partial(kernel, n_sp, n_tp),
        out_shape=jax.ShapeDtypeStruct((rows, width), BF16),
        in_specs=[hbm] * 18,
        out_specs=pl.BlockSpec(memory_space=pltpu.VMEM),
        scratch_shapes=[
            pltpu.VMEM((rows, width), BF16),
            pltpu.VMEM((1, width), F32),
            pltpu.VMEM(conv_taps.shape, F32),
            pltpu.VMEM((1, channels), F32),
            pltpu.VMEM((dirs * groups, per), F32),
            pltpu.VMEM((dirs * groups, per), F32),
            pltpu.VMEM((dirs * 2 * groups, per), F32),
            pltpu.SMEM((1, rows), F32),
            pltpu.VMEM((width * n_tp, 4 * channels), BF16),
            pltpu.VMEM((channels, width * n_tp), BF16),
            pltpu.VMEM((n_tp, channels, width), BF16),
            pltpu.VMEM((n_tp, rows, channels), BF16),
            pltpu.VMEM((rows, width), F32),
            pltpu.VMEM((2, dirs * groups * group, per), F32),
            pltpu.VMEM((2, dirs * groups * group, per), F32),
            pltpu.VMEM((n_tp, CHUNKS, rows, cw), BF16),
            pltpu.VMEM((n_tp, 1, width), F32),
            pltpu.VMEM((n_sp, 1, rows), F32),
            packed, packed, packed, packed, packed, packed, packed, packed, packed, packed,
            pltpu.VMEM((2, channels, states), BF16),
            pltpu.VMEM((2, channels, states), BF16),
            pltpu.VMEM((rows, channels), BF16),
            pltpu.VMEM((2, 16, channels), BF16),
            pltpu.VMEM((2, 8, 128), F32),
            pltpu.VMEM((n_sp, 2, 8, 128), F32),
            pltpu.VMEM((n_sp, 8, 128), F32),
            pltpu.VMEM((n_sp, 8, 128), F32),
        ] + [pltpu.VMEM((OUT_CHUNKS, rows, ow), BF16)] * 6 + [
            dma(18),
            dma(CHUNKS), dma(CHUNKS), dma(CHUNKS), dma(CHUNKS), dma(CHUNKS), dma(CHUNKS),
            dma(n_tp), dma(n_tp), dma(n_sp), dma(n_sp), dma(2), dma(2), dma(n_sp), dma(n_sp),
            dma(OUT_CHUNKS), dma(OUT_CHUNKS), dma(OUT_CHUNKS), dma(OUT_CHUNKS),
            dma(OUT_CHUNKS), dma(OUT_CHUNKS), dma(n_tp), dma(n_tp), dma(n_tp), dma(n_tp),
        ],
        compiler_params=pltpu.CompilerParams(
            collective_id=0, has_side_effects=True, vmem_limit_bytes=48 * 1024 * 1024),
    )(*(pltpu.with_memory_space_constraint(a, pltpu.HBM) for a in (
        stream, norm_gain.reshape(1, width), w_value, w_mix, w_gate, w_state, conv_taps,
        skip_gain.reshape(1, channels),
        decay_rate.reshape(dirs * groups, per), turn_rate.reshape(dirs * groups, per),
        rows_of(input_real), rows_of(input_imag),
        read_real.reshape(dirs * groups * group, per), read_imag.reshape(dirs * groups * group, per),
        initial_state.reshape(dirs * 2 * groups, per), intervals.reshape(1, rows),
        proj_conv, proj_state,
    )))


def solution(mesh):
    return jax.shard_map(
        functools.partial(per_device, mesh.shape["sp"], mesh.shape["tp"]),
        mesh=mesh,
        in_specs=(
            P("sp", "tp"), P("tp"), P(None, "tp"), P(None, "tp"), P(None, "tp"), P(None, "tp"),
            P(None, "tp"), P("tp"), P(None, "tp", None), P(None, "tp", None),
            P(None, "tp", None, None), P(None, "tp", None, None), P(None, "tp", None, None),
            P(None, "tp", None, None), P(None, None, "tp", None), P("sp"), P("tp", None),
            P("tp", None),
        ),
        out_specs=P("sp", "tp"),
        check_vma=False,
    )
```

```python
import functools

import jax
import jax.numpy as jnp
from jax import lax
from jax.experimental import pallas as pl
from jax.experimental.pallas import tpu as pltpu
from jax.sharding import PartitionSpec as P

EPSILON = 1e-06
MESH = pl.DeviceIdType.MESH
F32 = jnp.float32
BF16 = jnp.bfloat16
CHUNKS = 2
OUT_CHUNKS = 2


def dot(a, b):
    return jnp.dot(a, b, preferred_element_type=F32)


def dot_t(a, b):
    return lax.dot_general(a, b, (((1,), (1,)), ((), ())), preferred_element_type=F32)


def half_turns(angle):
    theta = 0.5 * angle
    n = jnp.floor(theta * 0.6366197723675814 + 0.5)
    r = theta - n * 1.5703125
    r = r - n * 0.00048351287841796875
    r = r - n * 3.1385570764541626e-07
    r = r - n * 6.077100627776710e-11
    odd = (n - 2.0 * jnp.floor(0.5 * n)) > 0.5
    z = r * r
    s = r + r * z * ((-1.9515295891e-4 * z + 8.3321608736e-3) * z - 1.6666654611e-1)
    c = 1.0 - 0.5 * z + z * z * (
        (2.443315711809948e-5 * z - 1.388731625493765e-3) * z + 4.166664568298827e-2
    )
    square = jnp.where(odd, c * c, s * s)
    double = 2.0 * s * c
    return square, jnp.where(odd, -double, double)


def expm1_of(x, e):
    p = 1.0 + x * (1.0 / 7.0)
    for k in (6.0, 5.0, 4.0, 3.0, 2.0):
        p = 1.0 + x * p * (1.0 / k)
    return jnp.where(x > -0.35, x * p, e - 1.0)


def repeat(lo, hi, body):
    if hi - lo <= 16:
        for i in range(lo, hi):
            body(i)
    else:
        def step(i, carry):
            body(i)
            return carry
        lax.fori_loop(lo, hi, step, 0)


def kernel(
    n_sp, n_tp,
    x_hbm, gain_hbm, wv, wm, wg, ws, taps_hbm, skip_hbm, decay_hbm, turn_hbm,
    inr, ini, rdr, rdi, init_hbm, iv_hbm, pc, ps,
    out_ref,
    x_ref, gain_ref, taps_ref, skip_ref, decay_ref, turn_ref, init_ref, iv_s,
    w_all, p_all, in_v, rd_v, x_full, gains, el_all, fr_ref, fi_ref, gr_ref, gi_ref,
    dr_ref, di_ref, h0r, h0i, h1r, h1i, bt_ref, rt_ref, src_ref, halo_ref, e_out, e_all,
    blk_r, blk_i, p1_out, p1_in, p2_out, p2_in, c_out, c_in,
    load_sem, as_sem, ar_sem, bs_sem, br_sem, fs_sem, fwr_sem, gs_sem, grv_sem,
    is_sem, ir_sem, hs_sem, hr_sem, es_sem, er_sem, p1s, p1r, p2s, p2r, cs, cr,
):
    tp, sp = lax.axis_index("tp"), lax.axis_index("sp")
    rows, width = x_hbm.shape
    channels = wv.shape[1]
    y, core = tp // 2, tp % 2
    sib = y * 2 + 1 - core
    oth = (1 - y) * 2 + core
    diag = (1 - y) * 2 + 1 - core
    cw = width // CHUNKS

    loads = []

    def load(src, dst):
        copy = pltpu.make_async_copy(src, dst, load_sem.at[len(loads)])
        copy.start()
        loads.append(copy)

    barrier = pltpu.get_barrier_semaphore()
    for j in range(1, n_tp):
        pl.semaphore_signal(barrier, inc=1, device_id={"tp": (tp + j) % n_tp}, device_id_type=MESH)
    repeat(1, n_sp, lambda r: pl.semaphore_signal(
        barrier, inc=1, device_id={"sp": (sp + r) % n_sp}, device_id_type=MESH))
    load(iv_hbm, iv_s)
    load(decay_hbm, decay_ref)
    load(turn_hbm, turn_ref)
    load(init_hbm, init_ref)
    load(inr, in_v.at[0])
    load(ini, in_v.at[1])
    load(rdr, rd_v.at[0])
    load(rdi, rd_v.at[1])
    load(x_hbm, x_ref)
    load(gain_hbm, gain_ref)
    for j, w in enumerate((wv, wm, wg, ws)):
        load(w, w_all.at[:, pl.ds(j * channels, channels)])
    load(taps_hbm, taps_ref)
    load(skip_hbm, skip_ref)
    load(pc, p_all.at[pl.ds(0, channels)])
    load(ps, p_all.at[pl.ds(channels, channels)])
    pl.semaphore_wait(barrier, n_tp - 1 + n_sp - 1)

    def remote(src, dst, send, recv, where):
        return pltpu.make_async_remote_copy(
            src_ref=src, dst_ref=dst, send_sem=send, recv_sem=recv,
            device_id=where, device_id_type=MESH)

    to_sib, to_oth, forward = [], [], []
    for c in range(CHUNKS):
        piece = x_hbm.at[:, pl.ds(c * cw, cw)]
        to_oth.append(remote(piece, x_full.at[tp, c], bs_sem.at[c], br_sem.at[c], {"tp": oth}))
        to_sib.append(remote(piece, x_full.at[tp, c], as_sem.at[c], ar_sem.at[c], {"tp": sib}))
        forward.append(remote(x_full.at[oth, c], x_full.at[oth, c], fs_sem.at[c], fwr_sem.at[c],
                              {"tp": sib}))
    gain_copies = [
        remote(gain_hbm, gains.at[tp], gs_sem.at[j], grv_sem.at[j], {"tp": (tp + j) % n_tp})
        for j in range(1, n_tp)
    ]
    for copy in gain_copies:
        copy.start()
    for c in range(CHUNKS):
        to_oth[c].start()
        to_sib[c].start()

    def interval_copy(r):
        return remote(iv_hbm, el_all.at[r], is_sem.at[r], ir_sem.at[r], {"sp": (sp + r) % n_sp})

    repeat(1, n_sp, lambda r: interval_copy(r).start())

    sub = lax.broadcasted_iota(jnp.int32, (8, 128), 0)
    top = sub < 4

    def pack(ref):
        even = ref[pl.ds(0, 8, stride=2), :]
        odd = ref[pl.ds(1, 8, stride=2), :]
        return jnp.concatenate([even, odd], axis=1)

    for i in range(4):
        loads[i].wait()
    decay, turn = pack(decay_ref), pack(turn_ref)

    def pack_init(part):
        halves = [
            jnp.concatenate([init_ref[pl.ds(d * 16 + part * 8, 4, stride=2), :],
                             init_ref[pl.ds(d * 16 + part * 8 + 1, 4, stride=2), :]], axis=1)
            for d in range(2)
        ]
        return jnp.concatenate(halves, axis=0)

    init_r, init_i = pack_init(0), pack_init(1)
    den = decay * decay + turn * turn
    td, dd = turn / den, decay / den

    def factors(k, carry):
        iv = jnp.where(top, iv_s[0, k], iv_s[0, rows - 1 - k])
        damp = -decay * iv
        square, sine = half_turns(turn * iv)
        e = jnp.exp(damp)
        cosine = 1.0 - 2.0 * square
        f_im = e * sine
        lift = expm1_of(damp, e) * cosine - 2.0 * square
        at = pl.ds(pl.multiple_of(k * 8, 8), 8)
        fr_ref[at, :] = e * cosine
        fi_ref[at, :] = f_im
        gr_ref[at, :] = td * f_im - dd * lift
        gi_ref[at, :] = -(dd * f_im + td * lift)
        return carry

    for c in range(CHUNKS):
        lax.fori_loop(c * rows // CHUNKS, (c + 1) * rows // CHUNKS, factors, 0, unroll=4)
        to_oth[c].wait_recv()
        forward[c].start()

    for i in range(4, 8):
        loads[i].wait()
    states = bt_ref.shape[2]
    per = rd_v.shape[2]
    half = states // 2
    group = channels * per // half
    spread = (lax.broadcasted_iota(jnp.int32, (per, half), 1) % per
              == lax.broadcasted_iota(jnp.int32, (per, half), 0)).astype(BF16)
    keep = ((lax.broadcasted_iota(jnp.int32, (channels, half), 1) // per)
            == (lax.broadcasted_iota(jnp.int32, (channels, half), 0) // group))
    for part in range(2):
        for d in range(2):
            at, to = pl.ds(d * channels, channels), pl.ds(d * half, half)
            wide = dot(in_v[part, at, :].astype(BF16), spread)
            bt_ref[part, :, to] = jnp.where(keep, wide, 0.0).astype(BF16)
            wide = dot(rd_v[part, at, :].astype(BF16), spread)
            if part:
                wide = -wide
            rt_ref[part, :, to] = jnp.where(keep, wide, 0.0).astype(BF16)

    for i in range(8, 14):
        loads[i].wait()
    for copy in gain_copies:
        copy.wait_recv()

    def project(value, gain, first):
        wide = value.astype(F32)
        scaled = (wide * gain).astype(BF16)
        term = dot(scaled, w_all[pl.ds(pl.multiple_of(first, cw), cw), :])
        return term, jnp.sum(wide * wide, axis=1, keepdims=True)

    projected = jnp.zeros((rows, 4 * channels), F32)
    squares = jnp.zeros((rows, 1), F32)
    for c in range(CHUNKS):
        t, s = project(x_ref[:, c * cw:(c + 1) * cw], gain_ref[:, c * cw:(c + 1) * cw],
                       tp * width + c * cw)
        projected, squares = projected + t, squares + s

    def remaining(owner, waits, projected, squares):
        for c in range(CHUNKS):
            if waits is not None:
                waits[c].wait_recv()
            t, s = project(x_full[owner, c], gains[owner][:, c * cw:(c + 1) * cw],
                           owner * width + c * cw)
            projected, squares = projected + t, squares + s
        return projected, squares

    projected, squares = remaining(sib, to_sib, projected, squares)
    projected, squares = remaining(oth, None, projected, squares)
    projected, squares = remaining(diag, forward, projected, squares)
    projected = projected * lax.rsqrt(squares / (width * n_tp) + EPSILON)
    conv_value = projected[:, :channels].astype(BF16).astype(F32)
    conv_mix = projected[:, channels:2 * channels].astype(BF16).astype(F32)
    conv_gate = projected[:, 2 * channels:3 * channels].astype(BF16).astype(F32)
    state_input = projected[:, 3 * channels:].astype(BF16)
    src_ref[...] = (conv_mix * conv_value).astype(BF16)

    for part, ref in ((0, dr_ref), (1, di_ref)):
        driven = dot(state_input, bt_ref[part])
        for j in range(8):
            ref[pl.ds(j, rows, stride=8), :] = driven[:, j * 128:(j + 1) * 128]

    halo_up = remote(src_ref.at[pl.ds(rows - 16, 16)], halo_ref.at[0], hs_sem.at[0], hr_sem.at[0],
                     {"sp": (sp + 1) % n_sp})
    halo_down = remote(src_ref.at[pl.ds(0, 16)], halo_ref.at[1], hs_sem.at[1], hr_sem.at[1],
                       {"sp": (sp + n_sp - 1) % n_sp})
    halo_up.start()
    halo_down.start()

    def first_pass(k, carry):
        hr, hi = carry
        at = pl.ds(pl.multiple_of(k * 8, 8), 8)
        back = pl.ds(pl.multiple_of((rows - 1 - k) * 8, 8), 8)
        dr = jnp.where(top, dr_ref[at, :], dr_ref[back, :])
        di = jnp.where(top, di_ref[at, :], di_ref[back, :])
        gr, gi = gr_ref[at, :], gi_ref[at, :]
        fr, fi = fr_ref[at, :], fi_ref[at, :]
        pr = gr * dr - gi * di
        pi = gr * di + gi * dr
        gr_ref[at, :] = pr
        gi_ref[at, :] = pi
        return fr * hr + (pr - fi * hi), fr * hi + (pi + fi * hr)

    zero = jnp.zeros((8, 128), F32)
    hr, hi = lax.fori_loop(0, rows, first_pass, (zero, zero), unroll=8)
    e_out[0] = hr
    e_out[1] = hi

    def edge_copy(r):
        return remote(e_out, e_all.at[r], es_sem.at[r], er_sem.at[r], {"sp": (sp + r) % n_sp})

    repeat(1, n_sp, lambda r: edge_copy(r).start())

    repeat(1, n_sp, lambda r: interval_copy(r).wait_recv())

    def block_factor(r):
        before = jnp.sum(el_all[r], axis=1, keepdims=True) * jnp.where(sp - r >= 0, 1.0, 0.0)
        after = jnp.sum(el_all[n_sp - r], axis=1, keepdims=True) * jnp.where(sp + r < n_sp, 1.0, 0.0)
        elapsed = jnp.where(top, before, after)
        square, sine = half_turns(turn * elapsed)
        e = jnp.exp(-decay * elapsed)
        blk_r[r] = e * (1.0 - 2.0 * square)
        blk_i[r] = e * sine

    repeat(1, n_sp, block_factor)

    halo_up.wait_recv()
    halo_down.wait_recv()
    for i in range(14, 18):
        loads[i].wait()
    source = src_ref[...].astype(F32)
    line = lax.broadcasted_iota(jnp.int32, (rows, channels), 0)
    before = halo_ref[0].astype(F32)[15:16, :] * jnp.where(sp > 0, 1.0, 0.0)
    after = halo_ref[1].astype(F32)[0:1, :] * jnp.where(sp < n_sp - 1, 1.0, 0.0)
    previous = jnp.where(line == 0, before, pltpu.roll(source, 1, 0))
    following = jnp.where(line == rows - 1, after, pltpu.roll(source, rows - 1, 0))
    filtered = taps_ref[0:1, :] * previous + taps_ref[1:2, :] * source + taps_ref[2:3, :] * following
    conv_out = (conv_gate * filtered).astype(BF16)

    repeat(1, n_sp, lambda r: edge_copy(r).wait_recv())

    def combine(r, hr, hi):
        er = jnp.where(top, jnp.where(sp - r >= 0, e_all[r, 0], 0.0),
                       jnp.where(sp + r < n_sp, e_all[n_sp - r, 0], 0.0))
        ei = jnp.where(top, jnp.where(sp - r >= 0, e_all[r, 1], 0.0),
                       jnp.where(sp + r < n_sp, e_all[n_sp - r, 1], 0.0))
        fr, fi = blk_r[r], blk_i[r]
        return fr * hr + (er - fi * hi), fr * hi + (ei + fi * hr)

    hr, hi = init_r, init_i
    if n_sp <= 16:
        for r in range(n_sp - 1, 0, -1):
            hr, hi = combine(r, hr, hi)
    else:
        hr, hi = lax.fori_loop(1, n_sp, lambda i, h: combine(n_sp - i, *h), (hr, hi))

    def second_pass(k, carry):
        hr, hi = carry
        at = pl.ds(pl.multiple_of(k * 8, 8), 8)
        back = pl.ds(pl.multiple_of((rows - 1 - k) * 8, 8), 8)
        fr, fi = fr_ref[at, :], fi_ref[at, :]
        nr = fr * hr + (gr_ref[at, :] - fi * hi)
        ni = fr * hi + (gi_ref[at, :] + fi * hr)
        h0r[at, :] = nr
        h0i[at, :] = ni
        h1r[back, :] = nr
        h1i[back, :] = ni
        return nr, ni

    lax.fori_loop(0, rows, second_pass, (hr, hi), unroll=8)

    response = state_input.astype(F32) * skip_ref[...]
    for part, (forth, back) in enumerate(((h0r, h1r), (h0i, h1i))):
        history = jnp.concatenate(
            [(forth if j < 4 else back)[pl.ds(j, rows, stride=8), :].astype(BF16) for j in range(8)],
            axis=1)
        response = response + dot_t(history, rt_ref[part])
    inner = 0.7978845608028654 * (response + 0.044715 * (response * response * response))
    state_out = (0.5 * response * (1.0 + jnp.tanh(inner))).astype(BF16)
    branches = jnp.concatenate([conv_out, state_out], axis=1)

    ow = width // OUT_CHUNKS

    def partial(owner, c):
        return dot(branches, p_all[:, pl.ds(pl.multiple_of(owner * width + c * ow, ow), ow)])

    first, second, cross = [], [], []
    for c in range(OUT_CHUNKS):
        p1_out[c] = partial(diag, c).astype(BF16)
        first.append(remote(p1_out.at[c], p1_in.at[c], p1s.at[c], p1r.at[c], {"tp": sib}))
        first[c].start()
    kept = [partial(oth, c) for c in range(OUT_CHUNKS)]
    for c in range(OUT_CHUNKS):
        first[c].wait_recv()
        c_out[c] = (kept[c] + p1_in[c].astype(F32)).astype(BF16)
        cross.append(remote(c_out.at[c], c_in.at[c], cs.at[c], cr.at[c], {"tp": oth}))
        cross[c].start()
    for c in range(OUT_CHUNKS):
        p2_out[c] = partial(sib, c).astype(BF16)
        second.append(remote(p2_out.at[c], p2_in.at[c], p2s.at[c], p2r.at[c], {"tp": sib}))
        second[c].start()
    mine = [partial(tp, c) for c in range(OUT_CHUNKS)]
    for c in range(OUT_CHUNKS):
        second[c].wait_recv()
        mine[c] = mine[c] + p2_in[c].astype(F32)
    for c in range(OUT_CHUNKS):
        cross[c].wait_recv()
        out_ref[:, c * ow:(c + 1) * ow] = (mine[c] + c_in[c].astype(F32)).astype(BF16)

    for copy in to_sib + to_oth + forward + gain_copies + [halo_up, halo_down] + first + second + cross:
        copy.wait_send()
    repeat(1, n_sp, lambda r: interval_copy(r).wait_send())
    repeat(1, n_sp, lambda r: edge_copy(r).wait_send())


def per_device(
    n_sp, n_tp,
    stream, norm_gain, w_value, w_mix, w_gate, w_state, conv_taps, skip_gain, decay_rate, turn_rate,
    input_real, input_imag, read_real, read_imag, initial_state, intervals, proj_conv, proj_state,
):
    rows, width = stream.shape
    channels = w_value.shape[1]
    dirs, groups, per, group = input_real.shape
    states = dirs * groups * per
    cw, ow = width // CHUNKS, width // OUT_CHUNKS
    hbm = pl.BlockSpec(memory_space=pltpu.HBM)
    dma = lambda n: pltpu.SemaphoreType.DMA((n,))
    packed = pltpu.VMEM((rows * 8, 128), F32)
    rows_of = lambda m: jnp.swapaxes(m, 2, 3).reshape(dirs * groups * group, per)
    return pl.pallas_call(
        functools.partial(kernel, n_sp, n_tp),
        out_shape=jax.ShapeDtypeStruct((rows, width), BF16),
        in_specs=[hbm] * 18,
        out_specs=pl.BlockSpec(memory_space=pltpu.VMEM),
        scratch_shapes=[
            pltpu.VMEM((rows, width), BF16),
            pltpu.VMEM((1, width), F32),
            pltpu.VMEM(conv_taps.shape, F32),
            pltpu.VMEM((1, channels), F32),
            pltpu.VMEM((dirs * groups, per), F32),
            pltpu.VMEM((dirs * groups, per), F32),
            pltpu.VMEM((dirs * 2 * groups, per), F32),
            pltpu.SMEM((1, rows), F32),
            pltpu.VMEM((width * n_tp, 4 * channels), BF16),
            pltpu.VMEM((2 * channels, width * n_tp), BF16),
            pltpu.VMEM((2, dirs * groups * group, per), F32),
            pltpu.VMEM((2, dirs * groups * group, per), F32),
            pltpu.VMEM((n_tp, CHUNKS, rows, cw), BF16),
            pltpu.VMEM((n_tp, 1, width), F32),
            pltpu.VMEM((n_sp, 1, rows), F32),
            packed, packed, packed, packed, packed, packed, packed, packed, packed, packed,
            pltpu.VMEM((2, channels, states), BF16),
            pltpu.VMEM((2, channels, states), BF16),
            pltpu.VMEM((rows, channels), BF16),
            pltpu.VMEM((2, 16, channels), BF16),
            pltpu.VMEM((2, 8, 128), F32),
            pltpu.VMEM((n_sp, 2, 8, 128), F32),
            pltpu.VMEM((n_sp, 8, 128), F32),
            pltpu.VMEM((n_sp, 8, 128), F32),
        ] + [pltpu.VMEM((OUT_CHUNKS, rows, ow), BF16)] * 6 + [
            dma(18),
            dma(CHUNKS), dma(CHUNKS), dma(CHUNKS), dma(CHUNKS), dma(CHUNKS), dma(CHUNKS),
            dma(n_tp), dma(n_tp), dma(n_sp), dma(n_sp), dma(2), dma(2), dma(n_sp), dma(n_sp),
            dma(OUT_CHUNKS), dma(OUT_CHUNKS), dma(OUT_CHUNKS), dma(OUT_CHUNKS),
            dma(OUT_CHUNKS), dma(OUT_CHUNKS),
        ],
        compiler_params=pltpu.CompilerParams(
            collective_id=0, has_side_effects=True, vmem_limit_bytes=48 * 1024 * 1024),
    )(*(pltpu.with_memory_space_constraint(a, pltpu.HBM) for a in (
        stream, norm_gain.reshape(1, width), w_value, w_mix, w_gate, w_state, conv_taps,
        skip_gain.reshape(1, channels),
        decay_rate.reshape(dirs * groups, per), turn_rate.reshape(dirs * groups, per),
        rows_of(input_real), rows_of(input_imag),
        read_real.reshape(dirs * groups * group, per), read_imag.reshape(dirs * groups * group, per),
        initial_state.reshape(dirs * 2 * groups, per), intervals.reshape(1, rows),
        proj_conv, proj_state,
    )))


def solution(mesh):
    return jax.shard_map(
        functools.partial(per_device, mesh.shape["sp"], mesh.shape["tp"]),
        mesh=mesh,
        in_specs=(
            P("sp", "tp"), P("tp"), P(None, "tp"), P(None, "tp"), P(None, "tp"), P(None, "tp"),
            P(None, "tp"), P("tp"), P(None, "tp", None), P(None, "tp", None),
            P(None, "tp", None, None), P(None, "tp", None, None), P(None, "tp", None, None),
            P(None, "tp", None, None), P(None, None, "tp", None), P("sp"), P("tp", None),
            P("tp", None),
        ),
        out_specs=P("sp", "tp"),
        check_vma=False,
    )
```
